512 devices in a mesh: ep: 128 (over z, x, core), tp: 4 (over y).
Axes of the slice: x: 4, y: 4, z: 16, core: 2. Of those that a mesh axis runs over, the one named last changes fastest.
Arguments:
- tokens: bfloat16 [1024, 2048], P('ep'), may hold values from -6 to 6
- norm_gain: float32 [2048], replicated, may hold values from 0.1 to 1.9
- query_weight: bfloat16 [2048, 1024], P('ep', 'tp'), may hold values from -0.125 to 0.125
- key_weight: bfloat16 [2048, 512], P('ep', 'tp'), may hold values from -0.125 to 0.125
- value_weight: bfloat16 [2048, 512], P('ep', 'tp'), may hold values from -0.125 to 0.125
- query_gain: float32 [64], replicated, may hold values from 0.9 to 1.9
- key_gain: float32 [64], replicated, may hold values from 0.9 to 1.9
- lambdas: float32 [8], P('tp'), may hold values from 0.3 to 0.8
- key_cache: bfloat16 [1024, 4, 320, 128], P('ep', 'tp'), may hold values from -5 to 5
- value_cache: bfloat16 [1024, 4, 320, 128], P('ep', 'tp'), may hold values from -6 to 6
- lengths: int32 [1024], P('ep'), may hold values from 1 to 320
- head_gain: float32 [128], replicated, may hold values from 0.1 to 1.9
- out_weight: bfloat16 [1024, 2048], P('tp', 'ep'), may hold values from -0.1875 to 0.1875
- ffn_gain: float32 [2048], replicated, may hold values from 0.1 to 1.9
- dense_gate_weight: bfloat16 [2048, 1024], P('ep', 'tp'), may hold values from -0.125 to 0.125
- dense_up_weight: bfloat16 [2048, 1024], P('ep', 'tp'), may hold values from -0.125 to 0.125
- dense_down_weight: bfloat16 [1024, 2048], P('tp', 'ep'), may hold values from -0.1875 to 0.1875
- branch_gate: float32 [2048], replicated, may hold values from -0.125 to 0.125
- expert_ids: int32 [1024, 2], P('ep'), may hold values from 0 to 15, all different within a row; in each aligned block of 8 rows (0 to 7, 8 to 15, ...) at most 2 rows name the same one
- expert_probs: float32 [1024, 2], P('ep'), may hold values from 0.1 to 0.9
- expert_gate: bfloat16 [128, 2048, 704], P('ep', None, 'tp'), may hold values from -0.125 to 0.125
- expert_up: bfloat16 [128, 2048, 704], P('ep', None, 'tp'), may hold values from -0.125 to 0.125
- expert_down: bfloat16 [128, 704, 2048], P('ep', 'tp'), may hold values from -0.078125 to 0.078125
Outputs:
- mixed: bfloat16 [1024, 2048], P('ep', 'tp')
The draws below stay inside these ranges and needn't reach their ends.
Inputs may be any that keep to these rules, and one draw needn't show every extreme that they name: `expert_ids`: each row names 2 different experts. Within each aligned block of 8 rows (the sequences of one index of ep) no expert is named more than 2 times, and in every draw some block names some expert exactly 2 times.
All inputs are finite; a program needn't handle non-finite values.
Results may differ from the reference program's by a relative error of at most 0.014.
Values may be sent and summed in bfloat16 or wider, within the bound.
No kernel may reach another device: no remote copies, remote signals or barrier semaphores. Data moves between devices by JAX's collectives and lax.ppermute only.
A program may use at most 64 MiB of HBM per device.

```python
import math
import jax
import jax.numpy as jnp
import numpy as np
from jax import lax

D = 2048
HQ = 8
KVH = 4
SUB = 64
VD = 128
FFD = 1024
EXPERTS = 16
FF = 5632
TOP = 2
SEQ_DEV = 8
CACHE = 320
SEQS = 1024
REP = 8
SLOTS = 128
CAP = 2
N_EP = 128
N_TP = 4


def set_ends(entries, own_key, low, top_value):
    longest = entries.shape.index(max(entries.shape))
    spots = []
    for shift in (0, 1):
        where = [jax.random.randint(jax.random.fold_in(own_key, axis), (), 0, length) for axis, length in enumerate(entries.shape)]
        where[longest] = (where[longest] + shift) % entries.shape[longest]
        spots.append(tuple(where))
    return entries.at[spots[0]].set(low).at[spots[1]].set(top_value)


def level_of(own_key, shape, split, least, top_value):
    level, own = 1.0, jax.random.fold_in(own_key, 6)
    for axis_at, shards_of in split:
        heights = jnp.exp(jax.random.uniform(jax.random.fold_in(own, axis_at), (shards_of,), jnp.float32, least / len(split), top_value / len(split)))
        level = level * jnp.repeat(heights, shape[axis_at] // shards_of).reshape([-1 if axis == axis_at else 1 for axis in range(len(shape))])
    return level


def routed_block(key, own, number, rows, amount, top, bound, skew):
    sequence = jax.random.permutation(key, amount)
    crowded, usual = load_shares(amount, rows * top, bound, skew, True), load_shares(amount, rows * top, bound, skew, False)
    places = jnp.arange(amount)

    def named(sizes, offset_by):
        used = int((sizes > 0).sum())
        fixed = max(1, used // 4)
        passed = fixed + (places - fixed + offset_by * (used - fixed)) % max(1, amount - fixed)
        return jnp.zeros((amount,), jnp.int32).at[sequence[jnp.where(places < fixed, places, passed)]].set(jnp.asarray(sizes, jnp.int32))

    sizes = jnp.where(number % 4 == 0, named(crowded, number // 4), named(usual, number - number // 4 - 1))
    mixed = jax.random.permutation(jax.random.fold_in(own, 3), amount)
    giver, receiver = mixed[0:amount // 2 * 2:2], mixed[1:amount // 2 * 2:2]
    room = jnp.minimum(sizes[giver] - 1, bound - sizes[receiver]) // 2
    room = jnp.where((giver == sequence[0]) | (receiver == sequence[0]) | (sizes[receiver] == 0), 0, jnp.maximum(room, 0))
    passed = jax.random.randint(jax.random.fold_in(own, 4), (amount // 2,), 0, 1 << 20) % (room + 1)
    sizes = sizes.at[giver].add(-passed).at[receiver].add(passed)
    members = jnp.searchsorted(jnp.cumsum(sizes), jnp.arange(rows * top), side="right").astype(jnp.int32)
    table = members.reshape(top, rows).T
    table = table[jax.random.permutation(jax.random.fold_in(own, 1), rows)]
    offset_by = jax.random.randint(jax.random.fold_in(own, 2), (rows, 1), 0, top)
    return jnp.take_along_axis(table, (jnp.arange(top)[None, :] + offset_by) % top, axis=1)


def load_shares(amount, total, reach, slope, full):
    weights = [(1 << 20) // math.isqrt(rank ** slope) + 1 for rank in range(1, amount + 1)]
    largest = reach if full else min(reach, max(-(-total // amount), total * weights[0] // sum(weights)))
    least = 1 if total - largest >= amount - 1 else 0
    given, surplus = [largest] + [least] * (amount - 1), total - largest - least * (amount - 1)
    while surplus > 0:
        free = [i for i in range(1, amount) if given[i] < largest] or [i for i in range(1, amount) if given[i] < reach]
        mass, budget = sum([weights[i] for i in free]), surplus
        for i in free:
            more = min(reach - given[i], max(1, budget * weights[i] // mass), surplus)
            given[i] = given[i] + more
            surplus = surplus - more
    return np.array(given)


def scatter_about(own_key, shape, deviation, limit, shards=(), kind=jnp.bfloat16):
    values = jax.random.normal(own_key, shape, jnp.float32) * deviation
    if len(shards) > 0:
        values = level_of(own_key, shape, shards, -0.22, 0.18) * values
    return jnp.clip(values, min=-limit, max=limit).astype(kind)


def setup_inputs(seed: int = 0) -> dict:
    splits = jax.random.split(jax.random.key(seed), 24)
    tokens = scatter_about(splits[0], (SEQS, D), 1.0, 6.0, ((0, 128),))
    norm_gain = jnp.clip(1.0 + 0.18 * jax.random.normal(splits[1], (D,), jnp.float32), 0.1, 1.9)
    query_weight = scatter_about(splits[2], (D, 2 * HQ * SUB), D ** -0.5, 0.125, ((0, 128), (1, 4)))
    key_weight = scatter_about(splits[3], (D, 2 * KVH * SUB), D ** -0.5, 0.125, ((0, 128), (1, 4)))
    value_weight = scatter_about(splits[4], (D, KVH * VD), D ** -0.5, 0.125, ((0, 128), (1, 4)))
    query_gain = jnp.clip(jnp.exp(jax.random.uniform(splits[5], (SUB,), jnp.float32, math.log(0.9), math.log(1.9))), 0.9, 1.9)
    key_gain = jnp.clip(jnp.exp(jax.random.uniform(splits[6], (SUB,), jnp.float32, math.log(0.9), math.log(1.9))), 0.9, 1.9)
    lambdas = jnp.clip(0.3 + 0.5 * jax.random.uniform(splits[7], (HQ,), jnp.float32) ** level_of(splits[7], (HQ,), ((0, 4),), -0.2, 0.2), 0.3, 0.8)
    key_cache = scatter_about(splits[8], (SEQS, KVH, CACHE, 2 * SUB), 1.0, 5.0, ((0, 128), (1, 4)))
    value_cache = scatter_about(splits[9], (SEQS, KVH, CACHE, VD), 1.0, 6.0, ((0, 128), (1, 4)))
    lengths = set_ends(jax.random.randint(splits[10], (SEQS,), 1, CACHE + 1), jax.random.fold_in(splits[10], 1), 1, CACHE).astype(jnp.int32)
    head_gain = jnp.clip(1.0 + 0.18 * jax.random.normal(splits[11], (VD,), jnp.float32), 0.1, 1.9)
    out_weight = scatter_about(splits[12], (HQ * VD, D), (HQ * VD) ** -0.5, 0.1875, ((0, 4), (1, 128)))
    ffn_gain = jnp.clip(1.0 + 0.18 * jax.random.normal(splits[13], (D,), jnp.float32), 0.1, 1.9)
    dense_gate_weight = scatter_about(splits[14], (D, FFD), D ** -0.5, 0.125, ((0, 128), (1, 4)))
    dense_up_weight = scatter_about(splits[15], (D, FFD), D ** -0.5, 0.125, ((0, 128), (1, 4)))
    dense_down_weight = scatter_about(splits[16], (FFD, D), FFD ** -0.5, 0.1875, ((0, 4), (1, 128)))
    branch_gate = scatter_about(splits[17], (D,), D ** -0.5, 0.125, (), jnp.float32)
    expert_ids_keys = jax.random.split(jax.random.fold_in(splits[18], 1), SEQS // SEQ_DEV)
    expert_ids_turns = jax.random.permutation(jax.random.fold_in(splits[18], 3), SEQS // SEQ_DEV)
    expert_ids = jax.vmap(lambda own, number: routed_block(jax.random.fold_in(splits[18], 2), own, number, SEQ_DEV, EXPERTS, TOP, CAP, 2))(expert_ids_keys, expert_ids_turns).reshape((SEQS, TOP))
    expert_probs = jnp.clip(0.1 + 0.79999997 * jax.random.uniform(splits[19], (SEQS, TOP), jnp.float32) ** level_of(splits[19], (SEQS, TOP), ((0, 128),), -0.2, 0.2), 0.1, 0.9)
    expert_gate = scatter_about(splits[20], (SLOTS, D, FF // REP), D ** -0.5, 0.125, ((0, 128), (2, 4)))
    expert_up = scatter_about(splits[21], (SLOTS, D, FF // REP), D ** -0.5, 0.125, ((0, 128), (2, 4)))
    expert_down = scatter_about(splits[22], (SLOTS, FF // REP, D), FF ** -0.5, 0.078125, ((0, 128), (1, 4)))
    return {"tokens": tokens, "norm_gain": norm_gain, "query_weight": query_weight, "key_weight": key_weight, "value_weight": value_weight, "query_gain": query_gain, "key_gain": key_gain, "lambdas": lambdas, "key_cache": key_cache, "value_cache": value_cache, "lengths": lengths, "head_gain": head_gain, "out_weight": out_weight, "ffn_gain": ffn_gain, "dense_gate_weight": dense_gate_weight, "dense_up_weight": dense_up_weight, "dense_down_weight": dense_down_weight, "branch_gate": branch_gate, "expert_ids": expert_ids, "expert_probs": expert_probs, "expert_gate": expert_gate, "expert_up": expert_up, "expert_down": expert_down}


epsilon = 1e-06

def rms_scale(values, scaling):
    return values * lax.rsqrt(lax.optimization_barrier(jnp.mean(values * values, axis=-1, keepdims=True)) + epsilon) * scaling

def settle(values):
    return lax.optimization_barrier(values.astype(jnp.bfloat16)).astype(jnp.float32)

def grouped_product(operand, weight, groups):
    seq_count = operand.shape[0]
    depth = operand.shape[1] // groups
    parts = operand.reshape(seq_count, groups, depth)
    blocks = weight.astype(jnp.float32).reshape(groups, depth, weight.shape[1])
    partial_value = settle(jnp.einsum('sgk,gkd->sgd', parts, blocks))
    return lax.optimization_barrier(jnp.sum(partial_value, axis=1))

def block_ranks(expert_ids):
    paired = expert_ids.reshape(N_EP, SEQ_DEV * TOP)
    onehot = (paired[:, :, None] == jnp.arange(EXPERTS, dtype=jnp.int32)[None, None, :]).astype(jnp.int32)
    earlier = (jnp.cumsum(onehot, axis=1) - onehot).astype(jnp.int32)
    return lax.optimization_barrier(jnp.sum(earlier * onehot, axis=2)).astype(jnp.int32).reshape(SEQS, TOP)

def reference(tokens, norm_gain, query_weight, key_weight, value_weight, query_gain, key_gain, lambdas, key_cache, value_cache, lengths, head_gain, out_weight, ffn_gain, dense_gate_weight, dense_up_weight, dense_down_weight, branch_gate, expert_ids, expert_probs, expert_gate, expert_up, expert_down):
    residual = tokens.astype(jnp.float32)
    normed = rms_scale(residual, norm_gain).astype(jnp.bfloat16)
    queries = settle(jnp.dot(normed, query_weight, preferred_element_type=jnp.float32))
    new_keys = settle(jnp.dot(normed, key_weight, preferred_element_type=jnp.float32))
    new_values = settle(jnp.dot(normed, value_weight, preferred_element_type=jnp.float32))
    per_group = HQ // KVH
    score_scale = SUB ** (-0.5)
    lam_heads = lambdas.reshape(1, KVH, per_group)

    def attend_block(inputs):
        block_queries, block_keys, block_values, block_cache, block_store, block_lengths = inputs
        seq_count = block_queries.shape[0]
        query_parts = settle(rms_scale(block_queries.reshape(seq_count, KVH, per_group, 2, SUB), query_gain))
        key_parts = settle(rms_scale(block_keys.reshape(seq_count, KVH, 2, SUB), key_gain))
        cached = settle(rms_scale(block_cache.astype(jnp.float32).reshape(seq_count, KVH, CACHE, 2, SUB), key_gain))
        scores = jnp.einsum('sgqcd,sgjcd->sgqcj', query_parts, cached) * score_scale
        own_score = jnp.einsum('sgqcd,sgcd->sgqc', query_parts, key_parts) * score_scale
        live_mask = jnp.arange(CACHE, dtype=jnp.int32)[None, :] < block_lengths[:, None]
        exponent = jnp.where(live_mask[:, None, None, None, :], jnp.exp(scores), 0.0)
        own_exponent = jnp.exp(own_score)
        denominator = lax.optimization_barrier(jnp.sum(exponent, axis=4)) + own_exponent
        shares = exponent / denominator[..., None]
        own_shares = own_exponent / denominator
        mixing = settle(shares[:, :, :, 0] - lam_heads[..., None] * shares[:, :, :, 1])
        own_mixing = settle(own_shares[:, :, :, 0] - lam_heads * own_shares[:, :, :, 1])
        head_out = jnp.einsum('sgqj,sgje->sgqe', mixing, block_store.astype(jnp.float32))
        head_out = head_out + own_mixing[..., None] * block_values.reshape(seq_count, KVH, VD)[:, :, None, :]
        return settle(rms_scale(head_out, head_gain)).reshape(seq_count, HQ * VD)
    blocks_in = (queries.reshape(N_EP, SEQ_DEV, -1), new_keys.reshape(N_EP, SEQ_DEV, -1), new_values.reshape(N_EP, SEQ_DEV, -1), key_cache.reshape(N_EP, SEQ_DEV, KVH, CACHE, 2 * SUB), value_cache.reshape(N_EP, SEQ_DEV, KVH, CACHE, VD), lengths.reshape(N_EP, SEQ_DEV))
    heads = lax.map(attend_block, blocks_in).reshape(SEQS, HQ * VD)
    attended = grouped_product(heads, out_weight, N_TP)
    middle = settle(residual + attended)
    ffn_input = settle(rms_scale(middle, ffn_gain))
    ffn_rows = ffn_input.astype(jnp.bfloat16)
    dense_gate = jnp.dot(ffn_rows, dense_gate_weight, preferred_element_type=jnp.float32)
    dense_up = jnp.dot(ffn_rows, dense_up_weight, preferred_element_type=jnp.float32)
    dense_hidden = settle(jax.nn.silu(dense_gate) * dense_up)
    dense_out = grouped_product(dense_hidden, dense_down_weight, N_TP)
    branch_weight = jax.nn.sigmoid(lax.optimization_barrier(jnp.sum(ffn_input * branch_gate, axis=1)))
    slot_ranks = block_ranks(expert_ids)
    rows_per = N_EP * CAP
    source = (jnp.arange(SEQS, dtype=jnp.int32) // SEQ_DEV)[:, None]
    slot_index = (expert_ids * rows_per + source * CAP + slot_ranks).astype(jnp.int32)
    slot_rows = jnp.zeros((EXPERTS * rows_per, D), jnp.bfloat16).at[slot_index.reshape(-1)].set(jnp.repeat(ffn_rows, TOP, axis=0))
    slot_rows = slot_rows.reshape(EXPERTS, rows_per, D)
    block_width = FF // REP
    piece_width = FF // (REP * N_TP)
    gate_slots = expert_gate.reshape(REP, EXPERTS, D, block_width)
    up_slots = expert_up.reshape(REP, EXPERTS, D, block_width)
    down_slots = expert_down.reshape(REP, EXPERTS, block_width, D)

    def one_expert(expert_index):
        rows_in = lax.dynamic_index_in_dim(slot_rows, expert_index, 0, False).astype(jnp.float32)
        gate_block = lax.dynamic_index_in_dim(gate_slots, expert_index, 1, False).astype(jnp.float32)
        up_block = lax.dynamic_index_in_dim(up_slots, expert_index, 1, False).astype(jnp.float32)
        down_block = lax.dynamic_index_in_dim(down_slots, expert_index, 1, False).astype(jnp.float32).reshape(REP, N_TP, piece_width, D)
        gate_val = jnp.einsum('rd,bdf->brf', rows_in, gate_block)
        up_val = jnp.einsum('rd,bdf->brf', rows_in, up_block)
        hidden = settle(jax.nn.silu(gate_val) * up_val).reshape(REP, rows_per, N_TP, piece_width)
        partial_value = settle(jnp.einsum('brtf,btfd->brtd', hidden, down_block))
        block_out = settle(lax.optimization_barrier(jnp.sum(partial_value, axis=2)))
        return lax.optimization_barrier(jnp.sum(block_out, axis=0))
    expert_out = lax.map(one_expert, jnp.arange(EXPERTS, dtype=jnp.int32)).reshape(EXPERTS * rows_per, D)
    picked = expert_out[slot_index]
    routed = lax.optimization_barrier(jnp.sum(expert_probs[:, :, None] * picked, axis=1))
    combined = middle + branch_weight[:, None] * dense_out + routed
    return combined.astype(jnp.bfloat16)
```

```python
import jax
import jax.numpy as jnp
from jax import lax
from jax.sharding import Mesh, PartitionSpec as P

SUB = 64
VD = 128
EXPERTS = 16
TOP = 2
CAP = 2


REP = 8
N_Z = 16
N_XC = 8
N_EP = 128
N_TP = 4
SEQ = 8
EP = ("b", "zp", "x", "c")
Z = ("b", "zp")
XC = ("x", "c")

epsilon = 1e-06


def rms_scale(values, scaling):
    return values * lax.rsqrt(jnp.mean(values * values, axis=-1, keepdims=True) + epsilon) * scaling


def exchange(values, axes):
    return lax.all_to_all(values, axes, split_axis=0, concat_axis=0, tiled=True)


def gather_small(values, axes, count):
    return exchange(jnp.broadcast_to(values[None], (count,) + values.shape), axes)


def to_mixed(rows):
    count = rows.shape[0]
    return rows.reshape(count, N_Z, N_XC, -1).transpose(0, 2, 1, 3).reshape(count, -1)


def from_mixed(rows):
    count = rows.shape[0]
    return rows.reshape(count, N_XC, N_Z, -1).transpose(0, 2, 1, 3).reshape(count, -1)


def attend(packed, key_cache, value_cache, lengths, query_gain, key_gain, lambdas, head_gain):
    seq_here = packed.shape[0]
    kv_here = key_cache.shape[1]
    cache_len = key_cache.shape[2]
    heads_here = lambdas.shape[0]
    per_group = heads_here // kv_here
    query_end = heads_here * 2 * SUB
    key_end = query_end + kv_here * 2 * SUB
    mixed = lax.optimization_barrier(packed.astype(jnp.bfloat16))
    query_parts = rms_scale(
        mixed[:, :query_end].astype(jnp.float32).reshape(seq_here, kv_here, per_group, 2, SUB),
        query_gain,
    ).astype(jnp.bfloat16)
    key_parts = rms_scale(
        mixed[:, query_end:key_end].astype(jnp.float32).reshape(seq_here, kv_here, 2, SUB), key_gain
    ).astype(jnp.bfloat16)
    new_values = mixed[:, key_end:].reshape(seq_here, kv_here, VD)
    cached = rms_scale(
        key_cache.astype(jnp.float32).reshape(seq_here, kv_here, cache_len, 2, SUB), key_gain
    ).astype(jnp.bfloat16)
    score_scale = SUB ** (-0.5)
    scores = (
        jnp.einsum("sgqcd,sgjcd->sgqcj", query_parts, cached, preferred_element_type=jnp.float32)
        * score_scale
    )
    own_score = (
        jnp.einsum("sgqcd,sgcd->sgqc", query_parts, key_parts, preferred_element_type=jnp.float32)
        * score_scale
    )
    live_mask = lax.broadcasted_iota(jnp.int32, (seq_here, cache_len), 1) < lengths[:, None]
    exponent = jnp.where(live_mask[:, None, None, None, :], jnp.exp(scores), 0.0)
    own_exponent = jnp.exp(own_score)
    denominator = jnp.sum(exponent, axis=4) + own_exponent
    shares = exponent / denominator[..., None]
    own_shares = own_exponent / denominator
    lam_heads = lambdas.reshape(1, kv_here, per_group)
    mixing = (shares[:, :, :, 0] - lam_heads[..., None] * shares[:, :, :, 1]).astype(jnp.bfloat16)
    own_mixing = lax.optimization_barrier(
        (own_shares[:, :, :, 0] - lam_heads * own_shares[:, :, :, 1]).astype(jnp.bfloat16)
    )
    head_out = jnp.einsum(
        "sgqj,sgje->sgqe", mixing, value_cache, preferred_element_type=jnp.float32
    )
    head_out = (
        head_out
        + own_mixing.astype(jnp.float32)[..., None] * new_values.astype(jnp.float32)[:, :, None, :]
    )
    return rms_scale(head_out, head_gain).astype(jnp.bfloat16).reshape(seq_here, heads_here * VD)


def route_tables(expert_ids, expert_probs):
    seq_here = expert_ids.shape[0]
    paired = expert_ids.reshape(-1)
    total_pairs = paired.shape[0]
    onehot = (paired[:, None] == lax.broadcasted_iota(jnp.int32, (total_pairs, EXPERTS), 1)).astype(
        jnp.float32
    )
    earlier = (
        lax.broadcasted_iota(jnp.int32, (total_pairs, total_pairs), 1)
        < lax.broadcasted_iota(jnp.int32, (total_pairs, total_pairs), 0)
    ).astype(jnp.float32)
    before = jnp.dot(earlier, onehot, precision=lax.Precision.HIGHEST)
    slot_ranks = jnp.sum(before * onehot, axis=1).astype(jnp.int32)
    slot_codes = (paired * CAP + slot_ranks).reshape(seq_here, TOP)
    slots_iota = lax.broadcasted_iota(jnp.int32, (seq_here, TOP, EXPERTS * CAP), 2)
    picked = (slot_codes[:, :, None] == slots_iota).astype(jnp.float32)
    select = jnp.sum(picked, axis=1)
    combine_weights = jnp.sum(picked * expert_probs[:, :, None], axis=1)
    return (select, combine_weights)


def own_columns(values, tp_start, share_width):
    return lax.dynamic_slice_in_dim(values, tp_start, share_width, 1)


def shards(
    tokens,
    norm_gain,
    query_weight,
    key_weight,
    value_weight,
    query_gain,
    key_gain,
    lambdas,
    key_cache,
    value_cache,
    lengths,
    head_gain,
    out_weight,
    ffn_gain,
    dense_gate_weight,
    dense_up_weight,
    dense_down_weight,
    branch_gate,
    expert_ids,
    expert_probs,
    expert_gate,
    expert_up,
    expert_down,
):
    residual = tokens.astype(jnp.float32)
    normed = rms_scale(residual, norm_gain).astype(jnp.bfloat16)
    width = residual.shape[1]
    share_width = width // N_TP
    tp_start = lax.axis_index("tp") * share_width

    spread = exchange(
        to_mixed(normed).reshape(SEQ, N_XC, width // N_XC).transpose(1, 0, 2), XC
    ).reshape(N_XC * SEQ, width // N_XC)
    shard = jnp.concatenate(
        (
            query_weight,
            key_weight,
            value_weight,
            out_weight.T,
            dense_gate_weight,
            dense_up_weight,
            dense_down_weight.T,
        ),
        axis=1,
    )
    held = lax.all_gather(shard, Z, axis=0, tiled=True)
    out_held = lax.all_gather(held[:, 512:768], XC, axis=0, tiled=True)
    dense_held = lax.all_gather(held[:, 768:], XC, axis=0, tiled=True)

    partial_rows = jnp.dot(spread, held[:, :512], preferred_element_type=jnp.float32)
    packed = jnp.sum(exchange(partial_rows.reshape(N_XC, SEQ, 512), XC), axis=0)
    head_out = attend(
        packed, key_cache, value_cache, lengths, query_gain, key_gain, lambdas, head_gain
    )
    attended_part = from_mixed(
        lax.dot_general(
            head_out, out_held, (((1,), (1,)), ((), ())), preferred_element_type=jnp.float32
        ).astype(jnp.bfloat16)
    )
    attended = jnp.sum(gather_small(attended_part, "tp", N_TP).astype(jnp.float32), axis=0)
    middle = lax.optimization_barrier((residual + attended).astype(jnp.bfloat16))
    middle_f32 = middle.astype(jnp.float32)
    ffn_input = lax.optimization_barrier(rms_scale(middle_f32, ffn_gain).astype(jnp.bfloat16))

    select, combine_weights = route_tables(expert_ids, expert_probs)
    ffn_share = own_columns(ffn_input, tp_start, share_width)
    chosen = jnp.dot(
        select.astype(jnp.bfloat16).T, ffn_share, preferred_element_type=jnp.float32
    ).astype(jnp.bfloat16)
    outgoing = jnp.broadcast_to(
        chosen.reshape(1, EXPERTS, CAP, share_width), (REP, EXPERTS, CAP, share_width)
    ).reshape(N_EP, CAP, share_width)
    incoming = exchange(outgoing, EP).reshape(N_EP * CAP, share_width)

    dense_both = jnp.dot(
        to_mixed(ffn_input), dense_held[:, :512], preferred_element_type=jnp.float32
    )
    dense_hidden = (jax.nn.silu(dense_both[:, :256]) * dense_both[:, 256:]).astype(jnp.bfloat16)
    dense_part = from_mixed(
        lax.dot_general(
            dense_hidden,
            dense_held[:, 512:],
            (((1,), (1,)), ((), ())),
            preferred_element_type=jnp.float32,
        ).astype(jnp.bfloat16)
    )
    branch_weight = jax.nn.sigmoid(
        jnp.sum(ffn_input.astype(jnp.float32) * branch_gate, axis=1, keepdims=True)
    )

    rows = gather_small(incoming, "tp", N_TP)
    rows = rows.transpose(1, 0, 2).reshape(N_EP * CAP, width)
    gate_val = jnp.dot(rows, expert_gate[0], preferred_element_type=jnp.float32)
    up_val = jnp.dot(rows, expert_up[0], preferred_element_type=jnp.float32)
    hidden = (jax.nn.silu(gate_val) * up_val).astype(jnp.bfloat16)
    expert_part = jnp.dot(hidden, expert_down[0], preferred_element_type=jnp.float32).astype(
        jnp.bfloat16
    )
    both_parts = jnp.concatenate((expert_part, dense_part), axis=0)
    both_parts = both_parts.reshape(N_EP * CAP + SEQ, N_TP, share_width).transpose(1, 0, 2)
    summed = jnp.sum(exchange(both_parts, "tp").astype(jnp.float32), axis=0)
    block_out = summed[: N_EP * CAP].astype(jnp.bfloat16).reshape(N_EP, CAP, share_width)
    dense = summed[N_EP * CAP :]
    returned = exchange(block_out, EP)
    expert_out = jnp.sum(
        returned.reshape(REP, EXPERTS * CAP, share_width).astype(jnp.float32), axis=0
    )
    routed = jnp.dot(combine_weights, expert_out, precision=lax.Precision.HIGHEST)
    combined = (
        own_columns(middle_f32, tp_start, share_width) + branch_weight * dense + routed
    )
    return combined.astype(jnp.bfloat16)


def solution(mesh):
    fine = Mesh(mesh.devices.reshape(8, 2, 4, 2, 4), ("b", "zp", "x", "c", "tp"))
    return jax.shard_map(
        shards,
        mesh=fine,
        in_specs=(
            P(EP, None),
            P(),
            P(EP, "tp"),
            P(EP, "tp"),
            P(EP, "tp"),
            P(),
            P(),
            P("tp"),
            P(EP, "tp", None, None),
            P(EP, "tp", None, None),
            P(EP),
            P(),
            P("tp", EP),
            P(),
            P(EP, "tp"),
            P(EP, "tp"),
            P("tp", EP),
            P(),
            P(EP, None),
            P(EP, None),
            P(EP, None, "tp"),
            P(EP, None, "tp"),
            P(EP, "tp", None),
        ),
        out_specs=P(EP, "tp"),
        check_vma=False,
    )
```

```python
import jax
import jax.numpy as jnp
from jax import lax
from jax.sharding import Mesh, PartitionSpec as P

SUB = 64
VD = 128
EXPERTS = 16
TOP = 2
CAP = 2


REP = 8
N_Z = 16
N_XC = 8
N_EP = 128
N_TP = 4
SEQ = 8
EP = ("b", "zp", "x", "c")
Z = ("b", "zp")
XC = ("x", "c")

epsilon = 1e-06


def rms_scale(values, scaling):
    return values * lax.rsqrt(jnp.mean(values * values, axis=-1, keepdims=True) + epsilon) * scaling


def mixed_scale(values, scaling):
    mean = jnp.mean(values * values, axis=(0, 2), keepdims=True)
    return values * lax.rsqrt(mean + epsilon) * scaling


def exchange(values, axes):
    return lax.all_to_all(values, axes, split_axis=0, concat_axis=0, tiled=True)


def gather_small(values, axes, count):
    return exchange(jnp.broadcast_to(values[None], (count,) + values.shape), axes)


def to_mixed(rows):
    count = rows.shape[0]
    return rows.reshape(count, N_Z, N_XC, -1).transpose(2, 0, 1, 3).reshape(N_XC, count, -1)


def from_mixed(rows):
    count = rows.shape[1]
    return rows.reshape(N_XC, count, N_Z, -1).transpose(1, 2, 0, 3).reshape(count, -1)


def attend(packed, key_cache, value_cache, lengths, query_gain, key_gain, lambdas, head_gain):
    seq_here = packed.shape[0]
    kv_here = key_cache.shape[1]
    cache_len = key_cache.shape[2]
    heads_here = lambdas.shape[0]
    per_group = heads_here // kv_here
    query_end = heads_here * 2 * SUB
    key_end = query_end + kv_here * 2 * SUB
    mixed = lax.optimization_barrier(packed.astype(jnp.bfloat16))
    query_parts = rms_scale(
        mixed[:, :query_end].astype(jnp.float32).reshape(seq_here, kv_here, per_group, 2, SUB),
        query_gain,
    ).astype(jnp.bfloat16)
    key_parts = rms_scale(
        mixed[:, query_end:key_end].astype(jnp.float32).reshape(seq_here, kv_here, 2, SUB), key_gain
    ).astype(jnp.bfloat16)
    new_values = mixed[:, key_end:].reshape(seq_here, kv_here, VD)
    cached = rms_scale(
        key_cache.astype(jnp.float32).reshape(seq_here, kv_here, cache_len, 2, SUB), key_gain
    ).astype(jnp.bfloat16)
    score_scale = SUB ** (-0.5)
    scores = (
        jnp.einsum("sgqcd,sgjcd->sgqcj", query_parts, cached, preferred_element_type=jnp.float32)
        * score_scale
    )
    own_score = (
        jnp.einsum("sgqcd,sgcd->sgqc", query_parts, key_parts, preferred_element_type=jnp.float32)
        * score_scale
    )
    live_mask = lax.broadcasted_iota(jnp.int32, (seq_here, cache_len), 1) < lengths[:, None]
    exponent = jnp.where(live_mask[:, None, None, None, :], jnp.exp(scores), 0.0)
    own_exponent = jnp.exp(own_score)
    denominator = jnp.sum(exponent, axis=4) + own_exponent
    shares = exponent / denominator[..., None]
    own_shares = own_exponent / denominator
    lam_heads = lambdas.reshape(1, kv_here, per_group)
    mixing = (shares[:, :, :, 0] - lam_heads[..., None] * shares[:, :, :, 1]).astype(jnp.bfloat16)
    own_mixing = lax.optimization_barrier(
        (own_shares[:, :, :, 0] - lam_heads * own_shares[:, :, :, 1]).astype(jnp.bfloat16)
    )
    head_out = jnp.einsum(
        "sgqj,sgje->sgqe", mixing, value_cache, preferred_element_type=jnp.float32
    )
    head_out = (
        head_out
        + own_mixing.astype(jnp.float32)[..., None] * new_values.astype(jnp.float32)[:, :, None, :]
    )
    return rms_scale(head_out, head_gain).astype(jnp.bfloat16).reshape(seq_here, heads_here * VD)


def route_tables(expert_ids, expert_probs):
    seq_here = expert_ids.shape[0]
    paired = expert_ids.reshape(-1)
    total_pairs = paired.shape[0]
    onehot = (paired[:, None] == lax.broadcasted_iota(jnp.int32, (total_pairs, EXPERTS), 1)).astype(
        jnp.float32
    )
    earlier = (
        lax.broadcasted_iota(jnp.int32, (total_pairs, total_pairs), 1)
        < lax.broadcasted_iota(jnp.int32, (total_pairs, total_pairs), 0)
    ).astype(jnp.float32)
    before = jnp.dot(earlier, onehot, precision=lax.Precision.HIGHEST)
    slot_ranks = jnp.sum(before * onehot, axis=1).astype(jnp.int32)
    slot_codes = (paired * CAP + slot_ranks).reshape(seq_here, TOP)
    slots_iota = lax.broadcasted_iota(jnp.int32, (seq_here, TOP, EXPERTS * CAP), 2)
    picked = (slot_codes[:, :, None] == slots_iota).astype(jnp.float32)
    select = jnp.sum(picked, axis=1)
    combine_weights = jnp.sum(picked * expert_probs[:, :, None], axis=1)
    lead_scale = jnp.sum(picked[:, 0] / expert_probs[:, :1], axis=0)
    return (select, combine_weights, lead_scale)


def split_pair(values):
    high = lax.reduce_precision(values, 8, 7)
    return high.astype(jnp.bfloat16), (values - high).astype(jnp.bfloat16)


def own_columns(values, tp_start, share_width):
    return lax.dynamic_slice_in_dim(values, tp_start, share_width, 1)


def shards(
    tokens,
    norm_gain,
    query_weight,
    key_weight,
    value_weight,
    query_gain,
    key_gain,
    lambdas,
    key_cache,
    value_cache,
    lengths,
    head_gain,
    out_weight,
    ffn_gain,
    dense_gate_weight,
    dense_up_weight,
    dense_down_weight,
    branch_gate,
    expert_ids,
    expert_probs,
    expert_gate,
    expert_up,
    expert_down,
):
    width = tokens.shape[1]
    share_width = width // N_TP
    tp_start = lax.axis_index("tp") * share_width
    block = width // N_XC

    residual = to_mixed(tokens).astype(jnp.float32)
    normed = mixed_scale(residual, to_mixed(norm_gain[None])).astype(jnp.bfloat16)
    with jax.named_scope("spread"):
        spread = exchange(normed, XC).reshape(N_XC * SEQ, block)
    shard = jnp.concatenate(
        (
            query_weight,
            key_weight,
            value_weight,
            out_weight.T,
            dense_gate_weight,
            dense_up_weight,
            dense_down_weight.T,
        ),
        axis=1,
    )
    with jax.named_scope("hold"):
        held = lax.all_gather(shard, Z, axis=0, tiled=True)

    partial_rows = jnp.dot(spread, held[:, :512], preferred_element_type=jnp.float32)
    with jax.named_scope("project"):
        packed = jnp.sum(exchange(partial_rows.reshape(N_XC, SEQ, 512), XC), axis=0)
    head_out = attend(
        packed, key_cache, value_cache, lengths, query_gain, key_gain, lambdas, head_gain
    )
    with jax.named_scope("heads"):
        all_heads = gather_small(head_out, XC, N_XC).reshape(N_XC * SEQ, 256)
    attended_part = lax.dot_general(
        all_heads, held[:, 512:768], (((1,), (1,)), ((), ())), preferred_element_type=jnp.float32
    ).astype(jnp.bfloat16)
    with jax.named_scope("attended"):
        parts = exchange(
            jnp.broadcast_to(
                attended_part.reshape(N_XC, 1, SEQ, block), (N_XC, N_TP, SEQ, block)
            ).reshape(N_XC * N_TP, SEQ, block),
            XC + ("tp",),
        ).reshape(N_XC, N_TP, SEQ, block)
    attended = jnp.sum(parts.astype(jnp.float32), axis=1)
    middle_mixed = lax.optimization_barrier((residual + attended).astype(jnp.bfloat16))
    ffn_input = from_mixed(
        mixed_scale(middle_mixed.astype(jnp.float32), to_mixed(ffn_gain[None])).astype(jnp.bfloat16)
    )
    middle = from_mixed(middle_mixed).astype(jnp.float32)

    select, combine_weights, lead_scale = route_tables(expert_ids, expert_probs)
    scale_high, scale_low = split_pair(lead_scale)
    tags = jnp.pad(jnp.stack((scale_high, scale_low), axis=1), ((0, 0), (0, 126)))
    ffn_share = own_columns(ffn_input, tp_start, share_width)
    chosen = jnp.dot(
        select.astype(jnp.bfloat16).T, ffn_share, preferred_element_type=jnp.float32
    ).astype(jnp.bfloat16)
    chosen = jnp.concatenate((chosen, tags), axis=1)
    sent = share_width + 128
    outgoing = jnp.broadcast_to(
        chosen.reshape(1, EXPERTS, CAP, sent), (REP, EXPERTS, CAP, sent)
    ).reshape(N_EP, CAP, sent)
    with jax.named_scope("route"):
        incoming = exchange(outgoing, EP).reshape(N_EP * CAP, sent)

    rep_start = lax.axis_index("b") * 32
    mine = jnp.concatenate(
        [
            lax.dynamic_slice_in_dim(held[:, start : start + 256], rep_start, 32, 1)
            for start in (768, 1024, 1280)
        ],
        axis=1,
    )
    with jax.named_scope("dense"):
        dense_held = lax.all_gather(mine, XC, axis=0, tiled=True)
    dense_held = (
        dense_held.reshape(N_XC, N_Z, 16, 96).transpose(1, 0, 2, 3).reshape(width, 96)
    )

    with jax.named_scope("join"):
        rows = gather_small(incoming[:, :share_width], "tp", N_TP)
    rows = rows.transpose(1, 0, 2).reshape(N_EP * CAP, width)
    tag = incoming[:, share_width : share_width + 2].astype(jnp.float32)
    branch_weight = jax.nn.sigmoid(
        jnp.sum(rows.astype(jnp.float32) * branch_gate, axis=1, keepdims=True)
    )
    dense_scale = branch_weight * (tag[:, :1] + tag[:, 1:])
    gate_val = jnp.dot(rows, expert_gate[0], preferred_element_type=jnp.float32)
    up_val = jnp.dot(rows, expert_up[0], preferred_element_type=jnp.float32)
    hidden = (jax.nn.silu(gate_val) * up_val).astype(jnp.bfloat16)
    dense_both = jnp.dot(rows, dense_held[:, :64], preferred_element_type=jnp.float32)
    dense_hidden = (
        jax.nn.silu(dense_both[:, :32]) * dense_both[:, 32:] * dense_scale
    ).astype(jnp.bfloat16)
    down = jnp.concatenate((expert_down[0], dense_held[:, 64:].T), axis=0)
    both_parts = jnp.dot(
        jnp.concatenate((hidden, dense_hidden), axis=1), down, preferred_element_type=jnp.float32
    ).astype(jnp.bfloat16)
    both_parts = both_parts.reshape(N_EP * CAP, N_TP, share_width).transpose(1, 0, 2)
    with jax.named_scope("reduce"):
        summed = jnp.sum(exchange(both_parts, "tp").astype(jnp.float32), axis=0)
    block_out = summed.astype(jnp.bfloat16).reshape(N_EP, CAP, share_width)
    with jax.named_scope("return"):
        returned = exchange(block_out, EP)
    expert_out = jnp.sum(
        returned.reshape(REP, EXPERTS * CAP, share_width).astype(jnp.float32), axis=0
    )
    routed = jnp.dot(combine_weights, expert_out, precision=lax.Precision.HIGHEST)
    return (own_columns(middle, tp_start, share_width) + routed).astype(jnp.bfloat16)


def solution(mesh):
    fine = Mesh(mesh.devices.reshape(8, 2, 4, 2, 4), ("b", "zp", "x", "c", "tp"))
    return jax.shard_map(
        shards,
        mesh=fine,
        in_specs=(
            P(EP, None),
            P(),
            P(EP, "tp"),
            P(EP, "tp"),
            P(EP, "tp"),
            P(),
            P(),
            P("tp"),
            P(EP, "tp", None, None),
            P(EP, "tp", None, None),
            P(EP),
            P(),
            P("tp", EP),
            P(),
            P(EP, "tp"),
            P(EP, "tp"),
            P("tp", EP),
            P(),
            P(EP, None),
            P(EP, None),
            P(EP, None, "tp"),
            P(EP, None, "tp"),
            P(EP, "tp", None),
        ),
        out_specs=P(EP, "tp"),
        check_vma=False,
    )
```

```python
import jax
import jax.numpy as jnp
from jax import lax
from jax.sharding import Mesh, PartitionSpec as P


SUB = 64
VD = 128
EXPERTS = 16
TOP = 2
CAP = 2


REP = 8
N_Z = 16
N_XC = 8
N_EP = 128
N_TP = 4
SEQ = 8
EP = ("b", "zp", "x", "c")
Z = ("b", "zp")
XC = ("x", "c")

epsilon = 1e-06


def rms_scale(values, scaling):
    return values * lax.rsqrt(jnp.mean(values * values, axis=-1, keepdims=True) + epsilon) * scaling


def mixed_scale(values, scaling):
    mean = jnp.mean(values * values, axis=(0, 2), keepdims=True)
    return values * lax.rsqrt(mean + epsilon) * scaling


def exchange(values, axes):
    return lax.all_to_all(values, axes, split_axis=0, concat_axis=0, tiled=True)


def gather_small(values, axes, count):
    return exchange(jnp.broadcast_to(values[None], (count,) + values.shape), axes)


def to_mixed(rows):
    count = rows.shape[0]
    return rows.reshape(count, N_Z, N_XC, -1).transpose(2, 0, 1, 3).reshape(N_XC, count, -1)


def from_mixed(rows):
    count = rows.shape[1]
    return rows.reshape(N_XC, count, N_Z, -1).transpose(1, 2, 0, 3).reshape(count, -1)


def attend(packed, key_cache, value_cache, lengths, query_gain, key_gain, lambdas, head_gain):
    seq_here = packed.shape[0]
    kv_here = key_cache.shape[1]
    cache_len = key_cache.shape[2]
    heads_here = lambdas.shape[0]
    per_group = heads_here // kv_here
    query_end = heads_here * 2 * SUB
    key_end = query_end + kv_here * 2 * SUB
    mixed = lax.optimization_barrier(packed.astype(jnp.bfloat16))
    query_parts = rms_scale(
        mixed[:, :query_end].astype(jnp.float32).reshape(seq_here, kv_here, per_group, 2, SUB),
        query_gain,
    ).astype(jnp.bfloat16)
    key_parts = rms_scale(
        mixed[:, query_end:key_end].astype(jnp.float32).reshape(seq_here, kv_here, 2, SUB), key_gain
    ).astype(jnp.bfloat16)
    new_values = mixed[:, key_end:].reshape(seq_here, kv_here, VD)
    cached = rms_scale(
        key_cache.astype(jnp.float32).reshape(seq_here, kv_here, cache_len, 2, SUB), key_gain
    ).astype(jnp.bfloat16)
    score_scale = SUB ** (-0.5)
    scores = (
        jnp.einsum("sgqcd,sgjcd->sgqcj", query_parts, cached, preferred_element_type=jnp.float32)
        * score_scale
    )
    own_score = (
        jnp.einsum("sgqcd,sgcd->sgqc", query_parts, key_parts, preferred_element_type=jnp.float32)
        * score_scale
    )
    live_mask = lax.broadcasted_iota(jnp.int32, (seq_here, cache_len), 1) < lengths[:, None]
    exponent = jnp.where(live_mask[:, None, None, None, :], jnp.exp(scores), 0.0)
    own_exponent = jnp.exp(own_score)
    denominator = jnp.sum(exponent, axis=4) + own_exponent
    shares = exponent / denominator[..., None]
    own_shares = own_exponent / denominator
    lam_heads = lambdas.reshape(1, kv_here, per_group)
    mixing = (shares[:, :, :, 0] - lam_heads[..., None] * shares[:, :, :, 1]).astype(jnp.bfloat16)
    own_mixing = lax.optimization_barrier(
        (own_shares[:, :, :, 0] - lam_heads * own_shares[:, :, :, 1]).astype(jnp.bfloat16)
    )
    head_out = jnp.einsum(
        "sgqj,sgje->sgqe", mixing, value_cache, preferred_element_type=jnp.float32
    )
    head_out = (
        head_out
        + own_mixing.astype(jnp.float32)[..., None] * new_values.astype(jnp.float32)[:, :, None, :]
    )
    return rms_scale(head_out, head_gain).astype(jnp.bfloat16).reshape(seq_here, heads_here * VD)


def route_tables(expert_ids, expert_probs):
    seq_here = expert_ids.shape[0]
    paired = expert_ids.reshape(-1)
    total_pairs = paired.shape[0]
    onehot = (paired[:, None] == lax.broadcasted_iota(jnp.int32, (total_pairs, EXPERTS), 1)).astype(
        jnp.float32
    )
    earlier = (
        lax.broadcasted_iota(jnp.int32, (total_pairs, total_pairs), 1)
        < lax.broadcasted_iota(jnp.int32, (total_pairs, total_pairs), 0)
    ).astype(jnp.float32)
    before = jnp.dot(earlier, onehot, precision=lax.Precision.HIGHEST)
    slot_ranks = jnp.sum(before * onehot, axis=1).astype(jnp.int32)
    slot_codes = (paired * CAP + slot_ranks).reshape(seq_here, TOP)
    slots_iota = lax.broadcasted_iota(jnp.int32, (seq_here, TOP, EXPERTS * CAP), 2)
    picked = (slot_codes[:, :, None] == slots_iota).astype(jnp.float32)
    select = jnp.sum(picked, axis=1)
    combine_weights = jnp.sum(picked * expert_probs[:, :, None], axis=1)
    lead_scale = jnp.sum(picked[:, 0] / expert_probs[:, :1], axis=0)
    return (select, combine_weights, lead_scale)


def split_pair(values):
    high = lax.reduce_precision(values, 8, 7)
    return high.astype(jnp.bfloat16), (values - high).astype(jnp.bfloat16)


def trade_columns(weight, tp_index):
    share = weight.shape[1] // N_TP
    kept = [own_columns(weight, tp_index * share, share)]
    for shift in (1, 2, 3):
        sent = own_columns(weight, ((tp_index + shift) & 3) * share, share)
        pairs = [(index, (index + shift) % N_TP) for index in range(N_TP)]
        kept.append(lax.ppermute(sent, "tp", pairs))
    kept = jnp.stack(kept)
    return jnp.concatenate(
        [
            lax.dynamic_index_in_dim(kept, (tp_index - index) & 3, 0, False)
            for index in range(N_TP)
        ],
        axis=0,
    )


def own_columns(values, tp_start, share_width):
    return lax.dynamic_slice_in_dim(values, tp_start, share_width, 1)


def shards(
    tokens,
    norm_gain,
    query_weight,
    key_weight,
    value_weight,
    query_gain,
    key_gain,
    lambdas,
    key_cache,
    value_cache,
    lengths,
    head_gain,
    out_weight,
    ffn_gain,
    dense_gate_weight,
    dense_up_weight,
    dense_down_weight,
    branch_gate,
    expert_ids,
    expert_probs,
    expert_gate,
    expert_up,
    expert_down,
):
    width = tokens.shape[1]
    share_width = width // N_TP
    tp_index = lax.axis_index("tp")
    tp_start = tp_index * share_width
    block = width // N_XC

    select, combine_weights, lead_scale = route_tables(expert_ids, expert_probs)
    tags = jnp.stack(split_pair(lead_scale), axis=1).reshape(2, 16, 2)
    tags = jnp.pad(tags, ((0, 0), (0, 0), (0, 30)))

    def by_rep(weight):
        return weight.reshape(16, REP, 32).transpose(1, 0, 2)

    shared = jnp.concatenate(
        (query_weight, key_weight, value_weight, out_weight.T), axis=1
    )
    dense_parts = jnp.concatenate(
        (by_rep(dense_gate_weight), by_rep(dense_up_weight), by_rep(dense_down_weight.T)), axis=2
    )
    message = jnp.concatenate(
        (
            jnp.broadcast_to(shared[None, None], (REP, 2, 16, 768)),
            jnp.broadcast_to(dense_parts[:, None], (REP, 2, 16, 96)),
            jnp.broadcast_to(tags[None], (REP, 2, 16, 32)),
        ),
        axis=3,
    ).reshape(N_Z, 16, 896)
    held = exchange(message, Z).reshape(N_Z * 16, 896)

    residual = to_mixed(tokens).astype(jnp.float32)
    normed = mixed_scale(residual, to_mixed(norm_gain[None])).astype(jnp.bfloat16)
    xc_index = lax.axis_index(XC)
    spread = lax.all_gather(normed, XC, axis=0)
    spread = lax.dynamic_index_in_dim(spread, xc_index, 1, False).reshape(N_XC * SEQ, block)

    partial_rows = jnp.dot(spread, held[:, :512], preferred_element_type=jnp.float32)
    packed = jnp.sum(exchange(partial_rows.reshape(N_XC, SEQ, 512), XC), axis=0)
    head_out = attend(
        packed, key_cache, value_cache, lengths, query_gain, key_gain, lambdas, head_gain
    )
    all_heads = gather_small(head_out, XC, N_XC).reshape(N_XC * SEQ, 256)
    attended_part = lax.dot_general(
        all_heads, held[:, 512:768], (((1,), (1,)), ((), ())), preferred_element_type=jnp.float32
    ).astype(jnp.bfloat16)
    parts = exchange(
        jnp.broadcast_to(
            attended_part.reshape(N_XC, 1, SEQ, block), (N_XC, N_TP, SEQ, block)
        ).reshape(N_XC * N_TP, SEQ, block),
        XC + ("tp",),
    ).reshape(N_XC, N_TP, SEQ, block)
    attended = jnp.sum(parts.astype(jnp.float32), axis=1)
    middle_mixed = lax.optimization_barrier((residual + attended).astype(jnp.bfloat16))
    ffn_input = from_mixed(
        mixed_scale(middle_mixed.astype(jnp.float32), to_mixed(ffn_gain[None])).astype(jnp.bfloat16)
    )
    middle = from_mixed(middle_mixed).astype(jnp.float32)

    ffn_share = own_columns(ffn_input, tp_start, share_width)
    chosen = jnp.dot(
        select.astype(jnp.bfloat16).T, ffn_share, preferred_element_type=jnp.float32
    ).astype(jnp.bfloat16)
    outgoing = jnp.broadcast_to(
        chosen.reshape(1, EXPERTS, CAP, share_width), (REP, EXPERTS, CAP, share_width)
    ).reshape(N_EP, CAP, share_width)
    incoming = exchange(outgoing, EP).reshape(N_EP * CAP, share_width)

    down = trade_columns(expert_down[0], tp_index)
    dense_held = lax.all_gather(held[:, 768:], XC, axis=0).reshape(N_XC, N_Z, 16, 128)
    incoming, dense_held = lax.optimization_barrier((incoming, dense_held))
    tag = lax.dynamic_slice_in_dim(dense_held, 2 * xc_index, CAP, 2)[..., 96:98]
    tag = jnp.sum(tag.transpose(1, 0, 2, 3).reshape(N_EP * CAP, 2).astype(jnp.float32), axis=1)
    dense_held = dense_held.transpose(1, 0, 2, 3).reshape(width, 128)
    dense_down = trade_columns(dense_held[:, 64:96].T, tp_index)

    rows = gather_small(incoming, "tp", N_TP)
    rows, dense_down = lax.optimization_barrier((rows, dense_down))
    rows = rows.transpose(1, 0, 2).reshape(N_EP * CAP, width)
    branch_weight = jax.nn.sigmoid(jnp.sum(rows.astype(jnp.float32) * branch_gate, axis=1))
    dense_scale = branch_weight * tag

    def units(weight):
        return lax.dot_general(
            weight, rows, (((0,), (1,)), ((), ())), preferred_element_type=jnp.float32
        )

    hidden = (jax.nn.silu(units(expert_gate[0])) * units(expert_up[0])).astype(jnp.bfloat16)
    dense_both = units(dense_held[:, :64])
    dense_hidden = (
        jax.nn.silu(dense_both[:32]) * dense_both[32:] * dense_scale[None]
    ).astype(jnp.bfloat16)
    all_hidden = gather_small(jnp.concatenate((hidden, dense_hidden), axis=0), "tp", N_TP)

    def summed(values, weight):
        return lax.dot_general(
            values.reshape(-1, N_EP * CAP),
            weight,
            (((0,), (0,)), ((), ())),
            preferred_element_type=jnp.float32,
        )

    block_out = summed(all_hidden[:, :176], down) + summed(all_hidden[:, 176:], dense_down)
    block_out = block_out.astype(jnp.bfloat16).reshape(N_EP, CAP, share_width)
    returned = exchange(block_out, EP)
    expert_out = jnp.sum(
        returned.reshape(REP, EXPERTS * CAP, share_width).astype(jnp.float32), axis=0
    )
    routed = jnp.dot(combine_weights, expert_out, precision=lax.Precision.HIGHEST)
    return (own_columns(middle, tp_start, share_width) + routed).astype(jnp.bfloat16)


def solution(mesh):
    fine = Mesh(mesh.devices.reshape(8, 2, 4, 2, 4), ("b", "zp", "x", "c", "tp"))
    return jax.shard_map(
        shards,
        mesh=fine,
        in_specs=(
            P(EP, None),
            P(),
            P(EP, "tp"),
            P(EP, "tp"),
            P(EP, "tp"),
            P(),
            P(),
            P("tp"),
            P(EP, "tp", None, None),
            P(EP, "tp", None, None),
            P(EP),
            P(),
            P("tp", EP),
            P(),
            P(EP, "tp"),
            P(EP, "tp"),
            P("tp", EP),
            P(),
            P(EP, None),
            P(EP, None),
            P(EP, None, "tp"),
            P(EP, None, "tp"),
            P(EP, "tp", None),
        ),
        out_specs=P(EP, "tp"),
        check_vma=False,
    )
```

```python
import jax
import jax.numpy as jnp
from jax import lax
from jax.experimental import pallas as pl
from jax.experimental.pallas import tpu as pltpu
from jax.sharding import Mesh, PartitionSpec as P

SUB = 64
VD = 128
EXPERTS = 16
TOP = 2
CAP = 2


REP = 8
N_Z = 16
N_XC = 8
N_EP = 128
N_TP = 4
SEQ = 8
EP = ("b", "zp", "x", "c")
Z = ("b", "zp")
XC = ("x", "c")

epsilon = 1e-06


def rms_scale(values, scaling):
    return values * lax.rsqrt(jnp.mean(values * values, axis=-1, keepdims=True) + epsilon) * scaling


def mixed_scale(values, scaling):
    mean = jnp.mean(values * values, axis=(0, 2), keepdims=True)
    return values * lax.rsqrt(mean + epsilon) * scaling


def exchange(values, axes):
    return lax.all_to_all(values, axes, split_axis=0, concat_axis=0, tiled=True)


def gather_small(values, axes, count):
    return exchange(jnp.broadcast_to(values[None], (count,) + values.shape), axes)


def to_mixed(rows):
    count = rows.shape[0]
    return rows.reshape(count, N_Z, N_XC, -1).transpose(2, 0, 1, 3).reshape(N_XC, count, -1)


def from_mixed(rows):
    count = rows.shape[1]
    return rows.reshape(N_XC, count, N_Z, -1).transpose(1, 2, 0, 3).reshape(count, -1)


def attend(packed, key_cache, value_cache, lengths, query_gain, key_gain, lambdas, head_gain):
    seq_here = packed.shape[0]
    kv_here = key_cache.shape[1]
    cache_len = key_cache.shape[2]
    heads_here = lambdas.shape[0]
    per_group = heads_here // kv_here
    query_end = heads_here * 2 * SUB
    key_end = query_end + kv_here * 2 * SUB
    mixed = lax.optimization_barrier(packed.astype(jnp.bfloat16))
    query_parts = rms_scale(
        mixed[:, :query_end].astype(jnp.float32).reshape(seq_here, kv_here, per_group, 2, SUB),
        query_gain,
    ).astype(jnp.bfloat16)
    key_parts = rms_scale(
        mixed[:, query_end:key_end].astype(jnp.float32).reshape(seq_here, kv_here, 2, SUB), key_gain
    ).astype(jnp.bfloat16)
    new_values = mixed[:, key_end:].reshape(seq_here, kv_here, VD)
    cached = rms_scale(
        key_cache.astype(jnp.float32).reshape(seq_here, kv_here, cache_len, 2, SUB), key_gain
    ).astype(jnp.bfloat16)
    score_scale = SUB ** (-0.5)
    scores = (
        jnp.einsum("sgqcd,sgjcd->sgqcj", query_parts, cached, preferred_element_type=jnp.float32)
        * score_scale
    )
    own_score = (
        jnp.einsum("sgqcd,sgcd->sgqc", query_parts, key_parts, preferred_element_type=jnp.float32)
        * score_scale
    )
    live_mask = lax.broadcasted_iota(jnp.int32, (seq_here, cache_len), 1) < lengths[:, None]
    exponent = jnp.where(live_mask[:, None, None, None, :], jnp.exp(scores), 0.0)
    own_exponent = jnp.exp(own_score)
    denominator = jnp.sum(exponent, axis=4) + own_exponent
    shares = exponent / denominator[..., None]
    own_shares = own_exponent / denominator
    lam_heads = lambdas.reshape(1, kv_here, per_group)
    mixing = (shares[:, :, :, 0] - lam_heads[..., None] * shares[:, :, :, 1]).astype(jnp.bfloat16)
    own_mixing = lax.optimization_barrier(
        (own_shares[:, :, :, 0] - lam_heads * own_shares[:, :, :, 1]).astype(jnp.bfloat16)
    )
    head_out = jnp.einsum(
        "sgqj,sgje->sgqe", mixing, value_cache, preferred_element_type=jnp.float32
    )
    head_out = (
        head_out
        + own_mixing.astype(jnp.float32)[..., None] * new_values.astype(jnp.float32)[:, :, None, :]
    )
    return rms_scale(head_out, head_gain).astype(jnp.bfloat16).reshape(seq_here, heads_here * VD)


def route_tables(expert_ids, expert_probs):
    seq_here = expert_ids.shape[0]
    paired = expert_ids.reshape(-1)
    total_pairs = paired.shape[0]
    onehot = (paired[:, None] == lax.broadcasted_iota(jnp.int32, (total_pairs, EXPERTS), 1)).astype(
        jnp.float32
    )
    earlier = (
        lax.broadcasted_iota(jnp.int32, (total_pairs, total_pairs), 1)
        < lax.broadcasted_iota(jnp.int32, (total_pairs, total_pairs), 0)
    ).astype(jnp.float32)
    before = jnp.dot(earlier, onehot, precision=lax.Precision.HIGHEST)
    slot_ranks = jnp.sum(before * onehot, axis=1).astype(jnp.int32)
    slot_codes = (paired * CAP + slot_ranks).reshape(seq_here, TOP)
    slots_iota = lax.broadcasted_iota(jnp.int32, (seq_here, TOP, EXPERTS * CAP), 2)
    picked = (slot_codes[:, :, None] == slots_iota).astype(jnp.float32)
    select = jnp.sum(picked, axis=1)
    combine_weights = jnp.sum(picked * expert_probs[:, :, None], axis=1)
    lead_scale = jnp.sum(picked[:, 0] / expert_probs[:, :1], axis=0)
    return (select, combine_weights, lead_scale)


def split_pair(values):
    high = lax.reduce_precision(values, 8, 7)
    return high.astype(jnp.bfloat16), (values - high).astype(jnp.bfloat16)


def message_body(query, key, value, out, gate, up, down, tags, message):
    lanes = lax.broadcasted_iota(jnp.int32, (16, 256), 1)
    shared = jnp.concatenate((query[...], key[...], value[...], out[...]), axis=1)
    wide = [part[...].astype(jnp.float32) for part in (gate, up, down)]
    for rep in range(REP):
        turned = [
            pltpu.roll(part, (32 * (place - rep)) % 256, 1) for place, part in enumerate(wide)
        ]
        own = jnp.where(
            lanes < 32, turned[0], jnp.where(lanes < 64, turned[1], turned[2])
        )[:, :128]
        own = jnp.where(lanes[:, :128] < 96, own, 0.0)
        for half in range(2):
            message[2 * rep + half, :, :768] = shared
            message[2 * rep + half, :, 768:] = (own + tags[half]).astype(jnp.bfloat16)


def build_message(*parts):
    return pl.pallas_call(
        message_body,
        out_shape=jax.ShapeDtypeStruct((N_Z, 16, 896), jnp.bfloat16),
        name="message",
    )(*parts)


def trade_columns(weight, tp_index):
    share = weight.shape[1] // N_TP
    kept = [own_columns(weight, tp_index * share, share)]
    for shift in (1, 2, 3):
        sent = own_columns(weight, ((tp_index + shift) & 3) * share, share)
        pairs = [(index, (index + shift) % N_TP) for index in range(N_TP)]
        kept.append(lax.ppermute(sent, "tp", pairs))
    return kept


def in_order(kept, tp_index):
    kept = jnp.stack(kept)
    return jnp.concatenate(
        [
            lax.dynamic_index_in_dim(kept, (tp_index - index) & 3, 0, False)
            for index in range(N_TP)
        ],
        axis=0,
    )


def own_columns(values, tp_start, share_width):
    return lax.dynamic_slice_in_dim(values, tp_start, share_width, 1)


def shards(
    tokens,
    norm_gain,
    query_weight,
    key_weight,
    value_weight,
    query_gain,
    key_gain,
    lambdas,
    key_cache,
    value_cache,
    lengths,
    head_gain,
    out_weight,
    ffn_gain,
    dense_gate_weight,
    dense_up_weight,
    dense_down_weight,
    branch_gate,
    expert_ids,
    expert_probs,
    expert_gate,
    expert_up,
    expert_down,
):
    width = tokens.shape[1]
    share_width = width // N_TP
    tp_index = lax.axis_index("tp")
    tp_start = tp_index * share_width
    block = width // N_XC

    select, combine_weights, lead_scale = route_tables(expert_ids, expert_probs)
    high, low = split_pair(lead_scale)
    tags = jnp.concatenate((high.reshape(2, 16, 1), low.reshape(2, 16, 1)), axis=2)
    tags = jnp.pad(tags.astype(jnp.float32), ((0, 0), (0, 0), (96, 30)))
    message = build_message(
        query_weight,
        key_weight,
        value_weight,
        out_weight.T,
        dense_gate_weight,
        dense_up_weight,
        dense_down_weight.T,
        tags,
    )
    held = exchange(message, Z).reshape(N_Z * 16, 896)
    down = trade_columns(expert_down[0], tp_index)
    held, down = lax.optimization_barrier((held, down))
    down = in_order(down, tp_index)
    dense_down = in_order(trade_columns(held[:, 832:864].T, tp_index), tp_index)

    residual = to_mixed(tokens).astype(jnp.float32)
    normed = mixed_scale(residual, to_mixed(norm_gain[None])).astype(jnp.bfloat16)
    xc_index = lax.axis_index(XC)
    spread = lax.all_gather(normed, XC, axis=0)
    spread = lax.dynamic_index_in_dim(spread, xc_index, 1, False).reshape(N_XC * SEQ, block)

    partial_rows = jnp.dot(spread, held[:, :512], preferred_element_type=jnp.float32)
    packed = jnp.sum(exchange(partial_rows.reshape(N_XC, SEQ, 512), XC), axis=0)
    head_out = attend(
        packed, key_cache, value_cache, lengths, query_gain, key_gain, lambdas, head_gain
    )
    all_heads = gather_small(head_out, XC, N_XC).reshape(N_XC * SEQ, 256)
    attended_part = lax.dot_general(
        all_heads, held[:, 512:768], (((1,), (1,)), ((), ())), preferred_element_type=jnp.float32
    ).astype(jnp.bfloat16)
    parts = exchange(
        jnp.broadcast_to(
            attended_part.reshape(N_XC, 1, SEQ, block), (N_XC, N_TP, SEQ, block)
        ).reshape(N_XC * N_TP, SEQ, block),
        XC + ("tp",),
    ).reshape(N_XC, N_TP, SEQ, block)
    parts, dense_down = lax.optimization_barrier((parts, dense_down))
    attended = jnp.sum(parts.astype(jnp.float32), axis=1)
    middle_mixed = lax.optimization_barrier((residual + attended).astype(jnp.bfloat16))
    ffn_input = from_mixed(
        mixed_scale(middle_mixed.astype(jnp.float32), to_mixed(ffn_gain[None])).astype(jnp.bfloat16)
    )
    middle = from_mixed(middle_mixed).astype(jnp.float32)

    ffn_share = own_columns(ffn_input, tp_start, share_width)
    chosen = jnp.dot(
        select.astype(jnp.bfloat16).T, ffn_share, preferred_element_type=jnp.float32
    ).astype(jnp.bfloat16)
    outgoing = jnp.broadcast_to(
        chosen.reshape(1, EXPERTS, CAP, share_width), (REP, EXPERTS, CAP, share_width)
    ).reshape(N_EP, CAP, share_width)
    incoming = exchange(outgoing, EP).reshape(N_EP * CAP, share_width)

    dense_held = jnp.concatenate((held[:, 768:], dense_down.T), axis=0)
    dense_held = lax.all_gather(dense_held, XC, axis=0)
    incoming, dense_held = lax.optimization_barrier((incoming, dense_held))
    dense_down = (
        dense_held[:, 256:].reshape(N_XC, 4, 16, 128).transpose(1, 0, 2, 3).reshape(512, 128)
    )
    dense_held = dense_held[:, :256].reshape(N_XC, N_Z, 16, 128)
    tag = lax.dynamic_slice_in_dim(dense_held, 2 * xc_index, CAP, 2)[..., 96:98]
    tag = jnp.sum(tag.transpose(1, 0, 2, 3).reshape(N_EP * CAP, 2).astype(jnp.float32), axis=1)
    dense_held = dense_held.transpose(1, 0, 2, 3).reshape(width, 128)[:, :64]

    rows = gather_small(incoming, "tp", N_TP)
    rows, dense_held, dense_down, tag = lax.optimization_barrier(
        (rows, dense_held, dense_down, tag)
    )
    rows = rows.transpose(1, 0, 2).reshape(N_EP * CAP, width)
    branch_weight = jax.nn.sigmoid(jnp.sum(rows.astype(jnp.float32) * branch_gate, axis=1))
    dense_scale = branch_weight * tag

    def units(weight):
        return lax.dot_general(
            weight, rows, (((0,), (1,)), ((), ())), preferred_element_type=jnp.float32
        )

    hidden = (jax.nn.silu(units(expert_gate[0])) * units(expert_up[0])).astype(jnp.bfloat16)
    dense_both = units(dense_held)
    dense_hidden = (
        jax.nn.silu(dense_both[:32]) * dense_both[32:] * dense_scale[None]
    ).astype(jnp.bfloat16)
    all_hidden = gather_small(jnp.concatenate((hidden, dense_hidden), axis=0), "tp", N_TP)

    def summed(values, weight):
        return lax.dot_general(
            values.reshape(-1, N_EP * CAP),
            weight,
            (((0,), (0,)), ((), ())),
            preferred_element_type=jnp.float32,
        )

    block_out = summed(all_hidden[:, :176], down) + summed(all_hidden[:, 176:], dense_down.T)
    block_out = block_out.astype(jnp.bfloat16).reshape(N_EP, CAP, share_width)
    returned = exchange(block_out, EP)
    expert_out = jnp.sum(
        returned.reshape(REP, EXPERTS * CAP, share_width).astype(jnp.float32), axis=0
    )
    routed = jnp.dot(combine_weights, expert_out, precision=lax.Precision.HIGHEST)
    return (own_columns(middle, tp_start, share_width) + routed).astype(jnp.bfloat16)


def solution(mesh):
    fine = Mesh(mesh.devices.reshape(8, 2, 4, 2, 4), ("b", "zp", "x", "c", "tp"))
    return jax.shard_map(
        shards,
        mesh=fine,
        in_specs=(
            P(EP, None),
            P(),
            P(EP, "tp"),
            P(EP, "tp"),
            P(EP, "tp"),
            P(),
            P(),
            P("tp"),
            P(EP, "tp", None, None),
            P(EP, "tp", None, None),
            P(EP),
            P(),
            P("tp", EP),
            P(),
            P(EP, "tp"),
            P(EP, "tp"),
            P("tp", EP),
            P(),
            P(EP, None),
            P(EP, None),
            P(EP, None, "tp"),
            P(EP, None, "tp"),
            P(EP, "tp", None),
        ),
        out_specs=P(EP, "tp"),
        check_vma=False,
    )
```

```python
import jax
import jax.numpy as jnp
from jax import lax
from jax.experimental import pallas as pl
from jax.experimental.pallas import tpu as pltpu
from jax.sharding import Mesh, PartitionSpec as P


SUB = 64
VD = 128
EXPERTS = 16
TOP = 2
CAP = 2


REP = 8
N_Z = 16
N_XC = 8
N_EP = 128
N_TP = 4
SEQ = 8
EP = ("b", "zp", "x", "c")
Z = ("b", "zp")
XC = ("x", "c")

epsilon = 1e-06


def rms_scale(values, scaling):
    return values * lax.rsqrt(jnp.mean(values * values, axis=-1, keepdims=True) + epsilon) * scaling


def mixed_scale(values, scaling):
    mean = jnp.mean(values * values, axis=(0, 2), keepdims=True)
    return values * lax.rsqrt(mean + epsilon) * scaling


def exchange(values, axes):
    return lax.all_to_all(values, axes, split_axis=0, concat_axis=0, tiled=True)


def gather_small(values, axes, count):
    return exchange(jnp.broadcast_to(values[None], (count,) + values.shape), axes)


def to_mixed(rows):
    count = rows.shape[0]
    return rows.reshape(count, N_Z, N_XC, -1).transpose(2, 0, 1, 3).reshape(N_XC, count, -1)


def from_mixed(rows):
    count = rows.shape[1]
    return rows.reshape(N_XC, count, N_Z, -1).transpose(1, 2, 0, 3).reshape(count, -1)


def attend(packed, key_cache, value_cache, lengths, query_gain, key_gain, lambdas, head_gain):
    seq_here = packed.shape[0]
    kv_here = key_cache.shape[1]
    cache_len = key_cache.shape[2]
    heads_here = lambdas.shape[0]
    per_group = heads_here // kv_here
    query_end = heads_here * 2 * SUB
    key_end = query_end + kv_here * 2 * SUB
    mixed = lax.optimization_barrier(packed.astype(jnp.bfloat16))
    query_parts = rms_scale(
        mixed[:, :query_end].astype(jnp.float32).reshape(seq_here, kv_here, per_group, 2, SUB),
        query_gain,
    ).astype(jnp.bfloat16)
    key_parts = rms_scale(
        mixed[:, query_end:key_end].astype(jnp.float32).reshape(seq_here, kv_here, 2, SUB), key_gain
    ).astype(jnp.bfloat16)
    new_values = mixed[:, key_end:].reshape(seq_here, kv_here, VD)
    cached = rms_scale(
        key_cache.astype(jnp.float32).reshape(seq_here, kv_here, cache_len, 2, SUB), key_gain
    ).astype(jnp.bfloat16)
    score_scale = SUB ** (-0.5)
    scores = (
        jnp.einsum("sgqcd,sgjcd->sgqcj", query_parts, cached, preferred_element_type=jnp.float32)
        * score_scale
    )
    own_score = (
        jnp.einsum("sgqcd,sgcd->sgqc", query_parts, key_parts, preferred_element_type=jnp.float32)
        * score_scale
    )
    live_mask = lax.broadcasted_iota(jnp.int32, (seq_here, cache_len), 1) < lengths[:, None]
    exponent = jnp.where(live_mask[:, None, None, None, :], jnp.exp(scores), 0.0)
    own_exponent = jnp.exp(own_score)
    denominator = jnp.sum(exponent, axis=4) + own_exponent
    shares = exponent / denominator[..., None]
    own_shares = own_exponent / denominator
    lam_heads = lambdas.reshape(1, kv_here, per_group)
    mixing = (shares[:, :, :, 0] - lam_heads[..., None] * shares[:, :, :, 1]).astype(jnp.bfloat16)
    own_mixing = lax.optimization_barrier(
        (own_shares[:, :, :, 0] - lam_heads * own_shares[:, :, :, 1]).astype(jnp.bfloat16)
    )
    head_out = jnp.einsum(
        "sgqj,sgje->sgqe", mixing, value_cache, preferred_element_type=jnp.float32
    )
    head_out = (
        head_out
        + own_mixing.astype(jnp.float32)[..., None] * new_values.astype(jnp.float32)[:, :, None, :]
    )
    return rms_scale(head_out, head_gain).astype(jnp.bfloat16).reshape(seq_here, heads_here * VD)


def route_tables(expert_ids, expert_probs):
    seq_here = expert_ids.shape[0]
    paired = expert_ids.reshape(-1)
    total_pairs = paired.shape[0]
    onehot = (paired[:, None] == lax.broadcasted_iota(jnp.int32, (total_pairs, EXPERTS), 1)).astype(
        jnp.float32
    )
    earlier = (
        lax.broadcasted_iota(jnp.int32, (total_pairs, total_pairs), 1)
        < lax.broadcasted_iota(jnp.int32, (total_pairs, total_pairs), 0)
    ).astype(jnp.float32)
    before = jnp.dot(earlier, onehot, precision=lax.Precision.HIGHEST)
    slot_ranks = jnp.sum(before * onehot, axis=1).astype(jnp.int32)
    slot_codes = (paired * CAP + slot_ranks).reshape(seq_here, TOP)
    slots_iota = lax.broadcasted_iota(jnp.int32, (seq_here, TOP, EXPERTS * CAP), 2)
    picked = (slot_codes[:, :, None] == slots_iota).astype(jnp.float32)
    select = jnp.sum(picked, axis=1)
    combine_weights = jnp.sum(picked * expert_probs[:, :, None], axis=1)
    return (select, combine_weights)


def message_body(ids, probs, query, key, value, out, gate, up, down, message):
    lanes = lax.broadcasted_iota(jnp.int32, (16, 256), 1)
    narrow = lax.broadcasted_iota(jnp.int32, (16, 128), 1)
    places = lax.broadcasted_iota(jnp.int32, (16, 128), 0)
    shared = jnp.concatenate((query[...], key[...], value[...], out[...]), axis=1)
    wide = [part[...].astype(jnp.float32) for part in (gate, up, down)]
    tags = [jnp.zeros((16, 128), jnp.float32) for _ in range(2)]
    for row in range(SEQ):
        chosen = ids[0, row]
        rank = jnp.int32(0)
        for earlier in range(row):
            for choice in range(TOP):
                rank = rank + (ids[choice, earlier] == chosen).astype(jnp.int32)
        slot = chosen * CAP + rank
        for half in range(2):
            tags[half] = jnp.where(places + 16 * half == slot, probs[0, row], tags[half])
    for half in range(2):
        used = tags[half] > 0.0
        inverse = jnp.where(used, 1.0 / jnp.where(used, tags[half], 1.0), 0.0)
        high = inverse.astype(jnp.bfloat16).astype(jnp.float32)
        tags[half] = jnp.where(
            narrow == 96, high, jnp.where(narrow == 97, inverse - high, 0.0)
        )
    for rep in range(REP):
        turned = [
            pltpu.roll(part, (32 * (place - rep)) % 256, 1) for place, part in enumerate(wide)
        ]
        own = jnp.where(
            lanes < 32, turned[0], jnp.where(lanes < 64, turned[1], turned[2])
        )[:, :128]
        own = jnp.where(narrow < 96, own, 0.0)
        for half in range(2):
            message[2 * rep + half, :, :768] = shared
            message[2 * rep + half, :, 768:] = (own + tags[half]).astype(jnp.bfloat16)


def build_message(ids, probs, *parts):
    scalars = pl.BlockSpec(memory_space=pltpu.SMEM)
    whole = pl.BlockSpec(memory_space=pltpu.VMEM)
    return pl.pallas_call(
        message_body,
        in_specs=[scalars, scalars] + [whole] * len(parts),
        out_shape=jax.ShapeDtypeStruct((N_Z, 16, 896), jnp.bfloat16),
        name="message",
    )(ids, probs, *parts)


def trade_columns(weight, tp_index):
    share = weight.shape[1] // N_TP
    kept = [own_columns(weight, tp_index * share, share)]
    for shift in (1, 2, 3):
        sent = own_columns(weight, ((tp_index + shift) & 3) * share, share)
        pairs = [(index, (index + shift) % N_TP) for index in range(N_TP)]
        kept.append(lax.ppermute(sent, "tp", pairs))
    return kept


def in_order(kept, tp_index):
    kept = jnp.stack(kept)
    return jnp.concatenate(
        [
            lax.dynamic_index_in_dim(kept, (tp_index - index) & 3, 0, False)
            for index in range(N_TP)
        ],
        axis=0,
    )


def own_columns(values, tp_start, share_width):
    return lax.dynamic_slice_in_dim(values, tp_start, share_width, 1)


def shards(
    tokens,
    norm_gain,
    query_weight,
    key_weight,
    value_weight,
    query_gain,
    key_gain,
    lambdas,
    key_cache,
    value_cache,
    lengths,
    head_gain,
    out_weight,
    ffn_gain,
    dense_gate_weight,
    dense_up_weight,
    dense_down_weight,
    branch_gate,
    expert_ids,
    expert_probs,
    expert_gate,
    expert_up,
    expert_down,
):
    width = tokens.shape[1]
    share_width = width // N_TP
    tp_index = lax.axis_index("tp")
    tp_start = tp_index * share_width
    block = width // N_XC

    select, combine_weights = route_tables(expert_ids, expert_probs)
    message = build_message(
        expert_ids.T,
        expert_probs.T,
        query_weight,
        key_weight,
        value_weight,
        out_weight.T,
        dense_gate_weight,
        dense_up_weight,
        dense_down_weight.T,
    )
    held = exchange(message, Z).reshape(N_Z * 16, 896)
    dense_down = in_order(trade_columns(held[:, 832:864].T, tp_index), tp_index)

    residual = to_mixed(tokens).astype(jnp.float32)
    normed = mixed_scale(residual, to_mixed(norm_gain[None])).astype(jnp.bfloat16)
    xc_index = lax.axis_index(XC)
    spread = lax.all_gather(normed, XC, axis=0)
    spread = lax.dynamic_index_in_dim(spread, xc_index, 1, False).reshape(N_XC * SEQ, block)

    partial_rows = jnp.dot(spread, held[:, :512], preferred_element_type=jnp.float32)
    packed = jnp.sum(exchange(partial_rows.reshape(N_XC, SEQ, 512), XC), axis=0)
    head_out = attend(
        packed, key_cache, value_cache, lengths, query_gain, key_gain, lambdas, head_gain
    )
    all_heads = gather_small(head_out, XC, N_XC).reshape(N_XC * SEQ, 256)
    attended_part = lax.dot_general(
        all_heads, held[:, 512:768], (((1,), (1,)), ((), ())), preferred_element_type=jnp.float32
    ).astype(jnp.bfloat16)
    parts = exchange(
        jnp.broadcast_to(
            attended_part.reshape(N_XC, 1, SEQ, block), (N_XC, N_TP, SEQ, block)
        ).reshape(N_XC * N_TP, SEQ, block),
        XC + ("tp",),
    ).reshape(N_XC, N_TP, SEQ, block)
    parts, dense_down = lax.optimization_barrier((parts, dense_down))
    attended = jnp.sum(parts.astype(jnp.float32), axis=1)
    middle_mixed = lax.optimization_barrier((residual + attended).astype(jnp.bfloat16))
    ffn_input = from_mixed(
        mixed_scale(middle_mixed.astype(jnp.float32), to_mixed(ffn_gain[None])).astype(jnp.bfloat16)
    )
    middle = from_mixed(middle_mixed).astype(jnp.float32)

    ffn_share = own_columns(ffn_input, tp_start, share_width)
    chosen = jnp.dot(
        select.astype(jnp.bfloat16).T, ffn_share, preferred_element_type=jnp.float32
    ).astype(jnp.bfloat16)
    outgoing = jnp.broadcast_to(
        chosen.reshape(1, EXPERTS, CAP, share_width), (REP, EXPERTS, CAP, share_width)
    ).reshape(N_EP, CAP, share_width)
    incoming = exchange(outgoing, EP).reshape(N_EP * CAP, share_width)

    down = in_order(trade_columns(expert_down[0], tp_index), tp_index)
    dense_held = jnp.concatenate((held[:, 768:], dense_down.T), axis=0)
    dense_held = lax.all_gather(dense_held, XC, axis=0)
    incoming, dense_held = lax.optimization_barrier((incoming, dense_held))
    dense_down = (
        dense_held[:, 256:].reshape(N_XC, 4, 16, 128).transpose(1, 0, 2, 3).reshape(512, 128)
    )
    dense_held = dense_held[:, :256].reshape(N_XC, N_Z, 16, 128)
    tag = lax.dynamic_slice_in_dim(dense_held, 2 * xc_index, CAP, 2)[..., 96:98]
    tag = jnp.sum(tag.transpose(1, 0, 2, 3).reshape(N_EP * CAP, 2).astype(jnp.float32), axis=1)
    dense_held = dense_held.transpose(1, 0, 2, 3).reshape(width, 128)[:, :64]

    rows = gather_small(incoming, "tp", N_TP)
    rows, dense_held, dense_down, tag = lax.optimization_barrier(
        (rows, dense_held, dense_down, tag)
    )
    rows = rows.transpose(1, 0, 2).reshape(N_EP * CAP, width)
    branch_weight = jax.nn.sigmoid(jnp.sum(rows.astype(jnp.float32) * branch_gate, axis=1))
    dense_scale = branch_weight * tag

    def units(weight):
        return lax.dot_general(
            weight, rows, (((0,), (1,)), ((), ())), preferred_element_type=jnp.float32
        )

    hidden = (jax.nn.silu(units(expert_gate[0])) * units(expert_up[0])).astype(jnp.bfloat16)
    dense_both = units(dense_held)
    dense_hidden = (
        jax.nn.silu(dense_both[:32]) * dense_both[32:] * dense_scale[None]
    ).astype(jnp.bfloat16)
    all_hidden = gather_small(jnp.concatenate((hidden, dense_hidden), axis=0), "tp", N_TP)

    def summed(values, weight):
        return lax.dot_general(
            values.reshape(-1, N_EP * CAP),
            weight,
            (((0,), (0,)), ((), ())),
            preferred_element_type=jnp.float32,
        )

    block_out = summed(all_hidden[:, :176], down) + summed(all_hidden[:, 176:], dense_down.T)
    block_out = block_out.astype(jnp.bfloat16).reshape(N_EP, CAP, share_width)
    returned = exchange(block_out, EP)
    expert_out = jnp.sum(
        returned.reshape(REP, EXPERTS * CAP, share_width).astype(jnp.float32), axis=0
    )
    routed = jnp.dot(combine_weights, expert_out, precision=lax.Precision.HIGHEST)
    return (own_columns(middle, tp_start, share_width) + routed).astype(jnp.bfloat16)


def solution(mesh):
    fine = Mesh(mesh.devices.reshape(8, 2, 4, 2, 4), ("b", "zp", "x", "c", "tp"))
    return jax.shard_map(
        shards,
        mesh=fine,
        in_specs=(
            P(EP, None),
            P(),
            P(EP, "tp"),
            P(EP, "tp"),
            P(EP, "tp"),
            P(),
            P(),
            P("tp"),
            P(EP, "tp", None, None),
            P(EP, "tp", None, None),
            P(EP),
            P(),
            P("tp", EP),
            P(),
            P(EP, "tp"),
            P(EP, "tp"),
            P("tp", EP),
            P(),
            P(EP, None),
            P(EP, None),
            P(EP, None, "tp"),
            P(EP, None, "tp"),
            P(EP, "tp", None),
        ),
        out_specs=P(EP, "tp"),
        check_vma=False,
    )
```

```python
import jax
import jax.numpy as jnp
from jax import lax
from jax.experimental import pallas as pl
from jax.experimental.pallas import tpu as pltpu
from jax.sharding import Mesh, PartitionSpec as P

SUB = 64
VD = 128
EXPERTS = 16
TOP = 2
CAP = 2


REP = 8
N_Z = 16
N_XC = 8
N_EP = 128
N_TP = 4
SEQ = 8
EP = ("b", "zp", "x", "c")
Z = ("b", "zp")
XC = ("x", "c")

epsilon = 1e-06


def rms_scale(values, scaling):
    return values * lax.rsqrt(jnp.mean(values * values, axis=-1, keepdims=True) + epsilon) * scaling


def mixed_scale(values, scaling):
    mean = jnp.mean(values * values, axis=(0, 2), keepdims=True)
    return values * lax.rsqrt(mean + epsilon) * scaling


def exchange(values, axes):
    return lax.all_to_all(values, axes, split_axis=0, concat_axis=0, tiled=True)


def gather_small(values, axes, count):
    return exchange(jnp.broadcast_to(values[None], (count,) + values.shape), axes)


def to_mixed(rows):
    count = rows.shape[0]
    return rows.reshape(count, N_Z, N_XC, -1).transpose(2, 0, 1, 3).reshape(N_XC, count, -1)


def from_mixed(rows):
    count = rows.shape[1]
    return rows.reshape(N_XC, count, N_Z, -1).transpose(1, 2, 0, 3).reshape(count, -1)


def attend(packed, key_cache, value_cache, lengths, query_gain, key_gain, lambdas, head_gain):
    seq_here = packed.shape[0]
    kv_here = key_cache.shape[1]
    cache_len = key_cache.shape[2]
    heads_here = lambdas.shape[0]
    per_group = heads_here // kv_here
    query_end = heads_here * 2 * SUB
    key_end = query_end + kv_here * 2 * SUB
    mixed = lax.optimization_barrier(packed.astype(jnp.bfloat16))
    query_parts = rms_scale(
        mixed[:, :query_end].astype(jnp.float32).reshape(seq_here, kv_here, per_group, 2, SUB),
        query_gain,
    ).astype(jnp.bfloat16)
    key_parts = rms_scale(
        mixed[:, query_end:key_end].astype(jnp.float32).reshape(seq_here, kv_here, 2, SUB), key_gain
    ).astype(jnp.bfloat16)
    new_values = mixed[:, key_end:].reshape(seq_here, kv_here, VD)
    cached = rms_scale(
        key_cache.astype(jnp.float32).reshape(seq_here, kv_here, cache_len, 2, SUB), key_gain
    ).astype(jnp.bfloat16)
    score_scale = SUB ** (-0.5)
    scores = (
        jnp.einsum("sgqcd,sgjcd->sgqcj", query_parts, cached, preferred_element_type=jnp.float32)
        * score_scale
    )
    own_score = (
        jnp.einsum("sgqcd,sgcd->sgqc", query_parts, key_parts, preferred_element_type=jnp.float32)
        * score_scale
    )
    live_mask = lax.broadcasted_iota(jnp.int32, (seq_here, cache_len), 1) < lengths[:, None]
    exponent = jnp.where(live_mask[:, None, None, None, :], jnp.exp(scores), 0.0)
    own_exponent = jnp.exp(own_score)
    denominator = jnp.sum(exponent, axis=4) + own_exponent
    shares = exponent / denominator[..., None]
    own_shares = own_exponent / denominator
    lam_heads = lambdas.reshape(1, kv_here, per_group)
    mixing = (shares[:, :, :, 0] - lam_heads[..., None] * shares[:, :, :, 1]).astype(jnp.bfloat16)
    own_mixing = lax.optimization_barrier(
        (own_shares[:, :, :, 0] - lam_heads * own_shares[:, :, :, 1]).astype(jnp.bfloat16)
    )
    head_out = jnp.einsum(
        "sgqj,sgje->sgqe", mixing, value_cache, preferred_element_type=jnp.float32
    )
    head_out = (
        head_out
        + own_mixing.astype(jnp.float32)[..., None] * new_values.astype(jnp.float32)[:, :, None, :]
    )
    return rms_scale(head_out, head_gain).astype(jnp.bfloat16).reshape(seq_here, heads_here * VD)


def route_tables(expert_ids, expert_probs):
    seq_here = expert_ids.shape[0]
    paired = expert_ids.reshape(-1)
    total_pairs = paired.shape[0]
    onehot = (paired[:, None] == lax.broadcasted_iota(jnp.int32, (total_pairs, EXPERTS), 1)).astype(
        jnp.float32
    )
    earlier = (
        lax.broadcasted_iota(jnp.int32, (total_pairs, total_pairs), 1)
        < lax.broadcasted_iota(jnp.int32, (total_pairs, total_pairs), 0)
    ).astype(jnp.float32)
    before = jnp.dot(earlier, onehot, precision=lax.Precision.HIGHEST)
    slot_ranks = jnp.sum(before * onehot, axis=1).astype(jnp.int32)
    slot_codes = (paired * CAP + slot_ranks).reshape(seq_here, TOP)
    slots_iota = lax.broadcasted_iota(jnp.int32, (seq_here, TOP, EXPERTS * CAP), 2)
    picked = (slot_codes[:, :, None] == slots_iota).astype(jnp.float32)
    select = jnp.sum(picked, axis=1)
    combine_weights = jnp.sum(picked * expert_probs[:, :, None], axis=1)
    return (select, combine_weights)


def message_body(ids, probs, query, key, value, out, gate, up, down, message):
    lanes = lax.broadcasted_iota(jnp.int32, (16, 256), 1)
    narrow = lax.broadcasted_iota(jnp.int32, (16, 128), 1)
    places = lax.broadcasted_iota(jnp.int32, (16, 128), 0)
    shared = jnp.concatenate((query[...], key[...], value[...], out[...]), axis=1)
    wide = [part[...].astype(jnp.float32) for part in (gate, up, down)]
    tags = [jnp.zeros((16, 128), jnp.float32) for _ in range(2)]
    for row in range(SEQ):
        chosen = ids[0, row]
        rank = jnp.int32(0)
        for earlier in range(row):
            for choice in range(TOP):
                rank = rank + (ids[choice, earlier] == chosen).astype(jnp.int32)
        slot = chosen * CAP + rank
        for half in range(2):
            tags[half] = jnp.where(places + 16 * half == slot, probs[0, row], tags[half])
    for half in range(2):
        used = tags[half] > 0.0
        inverse = jnp.where(used, 1.0 / jnp.where(used, tags[half], 1.0), 0.0)
        high = inverse.astype(jnp.bfloat16).astype(jnp.float32)
        tags[half] = jnp.where(
            narrow == 96, high, jnp.where(narrow == 97, inverse - high, 0.0)
        )
    for rep in range(REP):
        turned = [
            pltpu.roll(part, (32 * (place - rep)) % 256, 1) for place, part in enumerate(wide)
        ]
        own = jnp.where(
            lanes < 32, turned[0], jnp.where(lanes < 64, turned[1], turned[2])
        )[:, :128]
        own = jnp.where(narrow < 96, own, 0.0)
        for half in range(2):
            message[2 * rep + half, :, :768] = shared
            message[2 * rep + half, :, 768:] = (own + tags[half]).astype(jnp.bfloat16)


def build_message(ids, probs, *parts):
    scalars = pl.BlockSpec(memory_space=pltpu.SMEM)
    whole = pl.BlockSpec(memory_space=pltpu.VMEM)
    return pl.pallas_call(
        message_body,
        in_specs=[scalars, scalars] + [whole] * len(parts),
        out_shape=jax.ShapeDtypeStruct((N_Z, 16, 896), jnp.bfloat16),
        name="message",
    )(ids, probs, *parts)


def own_columns(values, tp_start, share_width):
    return lax.dynamic_slice_in_dim(values, tp_start, share_width, 1)


def shards(
    tokens,
    norm_gain,
    query_weight,
    key_weight,
    value_weight,
    query_gain,
    key_gain,
    lambdas,
    key_cache,
    value_cache,
    lengths,
    head_gain,
    out_weight,
    ffn_gain,
    dense_gate_weight,
    dense_up_weight,
    dense_down_weight,
    branch_gate,
    expert_ids,
    expert_probs,
    expert_gate,
    expert_up,
    expert_down,
):
    width = tokens.shape[1]
    share_width = width // N_TP
    tp_index = lax.axis_index("tp")
    tp_start = tp_index * share_width
    block = width // N_XC

    select, combine_weights = route_tables(expert_ids, expert_probs)
    message = build_message(
        expert_ids.T,
        expert_probs.T,
        query_weight,
        key_weight,
        value_weight,
        out_weight.T,
        dense_gate_weight,
        dense_up_weight,
        dense_down_weight.T,
    )
    with jax.named_scope("hold"):
        held = exchange(message, Z).reshape(N_Z * 16, 896)

    residual = to_mixed(tokens).astype(jnp.float32)
    normed = mixed_scale(residual, to_mixed(norm_gain[None])).astype(jnp.bfloat16)
    xc_index = lax.axis_index(XC)
    with jax.named_scope("spread"):
        spread = lax.all_gather(normed, XC, axis=0)
        spread = lax.dynamic_index_in_dim(spread, xc_index, 1, False).reshape(N_XC * SEQ, block)

    partial_rows = jnp.dot(spread, held[:, :512], preferred_element_type=jnp.float32)
    with jax.named_scope("project"):
        packed = jnp.sum(exchange(partial_rows.reshape(N_XC, SEQ, 512), XC), axis=0)
    head_out = attend(
        packed, key_cache, value_cache, lengths, query_gain, key_gain, lambdas, head_gain
    )
    with jax.named_scope("heads"):
        all_heads = gather_small(head_out, XC, N_XC).reshape(N_XC * SEQ, 256)
    attended_part = lax.dot_general(
        all_heads, held[:, 512:768], (((1,), (1,)), ((), ())), preferred_element_type=jnp.float32
    ).astype(jnp.bfloat16)
    with jax.named_scope("attended"):
        parts = exchange(
            jnp.broadcast_to(
                attended_part.reshape(N_XC, 1, SEQ, block), (N_XC, N_TP, SEQ, block)
            ).reshape(N_XC * N_TP, SEQ, block),
            XC + ("tp",),
        ).reshape(N_XC, N_TP, SEQ, block)
    attended = jnp.sum(parts.astype(jnp.float32), axis=1)
    middle_mixed = lax.optimization_barrier((residual + attended).astype(jnp.bfloat16))
    ffn_input = from_mixed(
        mixed_scale(middle_mixed.astype(jnp.float32), to_mixed(ffn_gain[None])).astype(jnp.bfloat16)
    )
    middle = from_mixed(middle_mixed).astype(jnp.float32)

    ffn_share = own_columns(ffn_input, tp_start, share_width)
    chosen = jnp.dot(
        select.astype(jnp.bfloat16).T, ffn_share, preferred_element_type=jnp.float32
    ).astype(jnp.bfloat16)
    outgoing = jnp.broadcast_to(
        chosen.reshape(1, EXPERTS, CAP, share_width), (REP, EXPERTS, CAP, share_width)
    ).reshape(N_EP, CAP, share_width)
    with jax.named_scope("route"):
        incoming = exchange(outgoing, EP).reshape(N_EP * CAP, share_width)

    with jax.named_scope("dense"):
        dense_held = lax.all_gather(held[:, 768:], XC, axis=0).reshape(N_XC, N_Z, 16, 128)
    incoming, dense_held = lax.optimization_barrier((incoming, dense_held))
    tag = lax.dynamic_slice_in_dim(dense_held, 2 * xc_index, CAP, 2)[..., 96:98]
    tag = jnp.sum(tag.transpose(1, 0, 2, 3).reshape(N_EP * CAP, 2).astype(jnp.float32), axis=1)
    dense_held = dense_held.transpose(1, 0, 2, 3).reshape(width, 128)
    down = jnp.concatenate((expert_down[0], dense_held[:, 64:96].T), axis=0)
    dense_held = dense_held[:, :64]

    with jax.named_scope("join"):
        rows = gather_small(incoming, "tp", N_TP)
    rows, dense_held, down, tag = lax.optimization_barrier((rows, dense_held, down, tag))
    rows = rows.transpose(1, 0, 2).reshape(N_EP * CAP, width)
    branch_weight = jax.nn.sigmoid(jnp.sum(rows.astype(jnp.float32) * branch_gate, axis=1))
    dense_scale = branch_weight * tag

    def units(weight):
        return lax.dot_general(
            weight, rows, (((0,), (1,)), ((), ())), preferred_element_type=jnp.float32
        )

    hidden = (jax.nn.silu(units(expert_gate[0])) * units(expert_up[0])).astype(jnp.bfloat16)
    dense_both = units(dense_held)
    dense_hidden = (
        jax.nn.silu(dense_both[:32]) * dense_both[32:] * dense_scale[None]
    ).astype(jnp.bfloat16)
    all_hidden = jnp.concatenate((hidden, dense_hidden), axis=0)
    parts = lax.dot_general(
        all_hidden, down, (((0,), (0,)), ((), ())), preferred_element_type=jnp.float32
    ).astype(jnp.bfloat16)
    parts = parts.reshape(N_EP * CAP, N_TP, share_width).transpose(1, 0, 2)
    with jax.named_scope("reduce"):
        block_out = jnp.sum(exchange(parts, "tp").astype(jnp.float32), axis=0)
    block_out = block_out.astype(jnp.bfloat16).reshape(N_EP, CAP, share_width)
    with jax.named_scope("return"):
        returned = exchange(block_out, EP)
    expert_out = jnp.sum(
        returned.reshape(REP, EXPERTS * CAP, share_width).astype(jnp.float32), axis=0
    )
    routed = jnp.dot(combine_weights, expert_out, precision=lax.Precision.HIGHEST)
    return (own_columns(middle, tp_start, share_width) + routed).astype(jnp.bfloat16)


def solution(mesh):
    fine = Mesh(mesh.devices.reshape(8, 2, 4, 2, 4), ("b", "zp", "x", "c", "tp"))
    return jax.shard_map(
        shards,
        mesh=fine,
        in_specs=(
            P(EP, None),
            P(),
            P(EP, "tp"),
            P(EP, "tp"),
            P(EP, "tp"),
            P(),
            P(),
            P("tp"),
            P(EP, "tp", None, None),
            P(EP, "tp", None, None),
            P(EP),
            P(),
            P("tp", EP),
            P(),
            P(EP, "tp"),
            P(EP, "tp"),
            P("tp", EP),
            P(),
            P(EP, None),
            P(EP, None),
            P(EP, None, "tp"),
            P(EP, None, "tp"),
            P(EP, "tp", None),
        ),
        out_specs=P(EP, "tp"),
        check_vma=False,
    )
```

```python
import jax
import jax.numpy as jnp
from jax import lax
from jax.experimental import pallas as pl
from jax.experimental.pallas import tpu as pltpu
from jax.sharding import Mesh, PartitionSpec as P

SUB = 64
VD = 128
EXPERTS = 16
TOP = 2
CAP = 2


REP = 8
N_Z = 16
N_XC = 8
N_EP = 128
N_TP = 4
SEQ = 8
EP = ("b", "zp", "x", "c")
Z = ("b", "zp")
XC = ("x", "c")

epsilon = 1e-06


def rms_scale(values, scaling):
    return values * lax.rsqrt(jnp.mean(values * values, axis=-1, keepdims=True) + epsilon) * scaling


def mixed_scale(values, scaling):
    mean = jnp.mean(values * values, axis=(0, 2), keepdims=True)
    return values * lax.rsqrt(mean + epsilon) * scaling


def exchange(values, axes):
    return lax.all_to_all(values, axes, split_axis=0, concat_axis=0, tiled=True)


def gather_small(values, axes, count):
    return exchange(jnp.broadcast_to(values[None], (count,) + values.shape), axes)


def to_mixed(rows):
    count = rows.shape[0]
    return rows.reshape(count, N_Z, N_XC, -1).transpose(2, 0, 1, 3).reshape(N_XC, count, -1)


def from_mixed(rows):
    count = rows.shape[1]
    return rows.reshape(N_XC, count, N_Z, -1).transpose(1, 2, 0, 3).reshape(count, -1)


def attend(packed, key_cache, value_cache, lengths, query_gain, key_gain, lambdas, head_gain):
    seq_here = packed.shape[0]
    kv_here = key_cache.shape[1]
    cache_len = key_cache.shape[2]
    heads_here = lambdas.shape[0]
    per_group = heads_here // kv_here
    query_end = heads_here * 2 * SUB
    key_end = query_end + kv_here * 2 * SUB
    mixed = lax.optimization_barrier(packed.astype(jnp.bfloat16))
    query_parts = rms_scale(
        mixed[:, :query_end].astype(jnp.float32).reshape(seq_here, kv_here, per_group, 2, SUB),
        query_gain,
    ).astype(jnp.bfloat16)
    key_parts = rms_scale(
        mixed[:, query_end:key_end].astype(jnp.float32).reshape(seq_here, kv_here, 2, SUB), key_gain
    ).astype(jnp.bfloat16)
    new_values = mixed[:, key_end:].reshape(seq_here, kv_here, VD)
    cached = rms_scale(
        key_cache.astype(jnp.float32).reshape(seq_here, kv_here, cache_len, 2, SUB), key_gain
    ).astype(jnp.bfloat16)
    score_scale = SUB ** (-0.5)
    scores = (
        jnp.einsum("sgqcd,sgjcd->sgqcj", query_parts, cached, preferred_element_type=jnp.float32)
        * score_scale
    )
    own_score = (
        jnp.einsum("sgqcd,sgcd->sgqc", query_parts, key_parts, preferred_element_type=jnp.float32)
        * score_scale
    )
    live_mask = lax.broadcasted_iota(jnp.int32, (seq_here, cache_len), 1) < lengths[:, None]
    exponent = jnp.where(live_mask[:, None, None, None, :], jnp.exp(scores), 0.0)
    own_exponent = jnp.exp(own_score)
    denominator = jnp.sum(exponent, axis=4) + own_exponent
    shares = exponent / denominator[..., None]
    own_shares = own_exponent / denominator
    lam_heads = lambdas.reshape(1, kv_here, per_group)
    mixing = (shares[:, :, :, 0] - lam_heads[..., None] * shares[:, :, :, 1]).astype(jnp.bfloat16)
    own_mixing = lax.optimization_barrier(
        (own_shares[:, :, :, 0] - lam_heads * own_shares[:, :, :, 1]).astype(jnp.bfloat16)
    )
    head_out = jnp.einsum(
        "sgqj,sgje->sgqe", mixing, value_cache, preferred_element_type=jnp.float32
    )
    head_out = (
        head_out
        + own_mixing.astype(jnp.float32)[..., None] * new_values.astype(jnp.float32)[:, :, None, :]
    )
    return rms_scale(head_out, head_gain).astype(jnp.bfloat16).reshape(seq_here, heads_here * VD)


def route_tables(expert_ids, expert_probs):
    seq_here = expert_ids.shape[0]
    paired = expert_ids.reshape(-1)
    total_pairs = paired.shape[0]
    onehot = (paired[:, None] == lax.broadcasted_iota(jnp.int32, (total_pairs, EXPERTS), 1)).astype(
        jnp.float32
    )
    earlier = (
        lax.broadcasted_iota(jnp.int32, (total_pairs, total_pairs), 1)
        < lax.broadcasted_iota(jnp.int32, (total_pairs, total_pairs), 0)
    ).astype(jnp.float32)
    before = jnp.dot(earlier, onehot, precision=lax.Precision.HIGHEST)
    slot_ranks = jnp.sum(before * onehot, axis=1).astype(jnp.int32)
    slot_codes = (paired * CAP + slot_ranks).reshape(seq_here, TOP)
    slots_iota = lax.broadcasted_iota(jnp.int32, (seq_here, TOP, EXPERTS * CAP), 2)
    picked = (slot_codes[:, :, None] == slots_iota).astype(jnp.float32)
    select = jnp.sum(picked, axis=1)
    combine_weights = jnp.sum(picked * expert_probs[:, :, None], axis=1)
    return (select, combine_weights)


def message_body(ids, probs, query, key, value, out, gate, up, down, message):
    lanes = lax.broadcasted_iota(jnp.int32, (16, 256), 1)
    narrow = lax.broadcasted_iota(jnp.int32, (16, 128), 1)
    places = lax.broadcasted_iota(jnp.int32, (16, 128), 0)
    shared = jnp.concatenate((query[...], key[...], value[...]), axis=1)
    wide = [part[...].astype(jnp.float32) for part in (gate, up, down)]
    held = out[...].astype(jnp.float32)
    tags = [jnp.zeros((16, 128), jnp.float32) for _ in range(2)]
    for row in range(SEQ):
        chosen = ids[0, row]
        rank = jnp.int32(0)
        for earlier in range(row):
            for choice in range(TOP):
                rank = rank + (ids[choice, earlier] == chosen).astype(jnp.int32)
        slot = chosen * CAP + rank
        for half in range(2):
            tags[half] = jnp.where(places + 16 * half == slot, probs[0, row], tags[half])
    tagged = jnp.zeros((16, 128), jnp.float32)
    for half in range(2):
        used = tags[half] > 0.0
        inverse = jnp.where(used, 1.0 / jnp.where(used, tags[half], 1.0), 0.0)
        high = inverse.astype(jnp.bfloat16).astype(jnp.float32)
        tagged = jnp.where(narrow == 96 + 2 * half, high, tagged)
        tagged = jnp.where(narrow == 97 + 2 * half, inverse - high, tagged)
    for rep in range(REP):
        turned = [
            pltpu.roll(part, (32 * (place - rep)) % 256, 1) for place, part in enumerate(wide)
        ]
        own = jnp.where(
            lanes < 32, turned[0], jnp.where(lanes < 64, turned[1], turned[2])
        )[:, :128]
        own = jnp.where(narrow < 96, own, tagged)
        extra = jnp.concatenate((held, own, jnp.zeros((16, 128), jnp.float32)), axis=1)
        for half in range(2):
            message[2 * rep + half, :16, :] = shared
            message[2 * rep + half, 16:, :] = extra[8 * half : 8 * half + 8].astype(jnp.bfloat16)


def build_message(ids, probs, *parts):
    scalars = pl.BlockSpec(memory_space=pltpu.SMEM)
    whole = pl.BlockSpec(memory_space=pltpu.VMEM)
    return pl.pallas_call(
        message_body,
        in_specs=[scalars, scalars] + [whole] * len(parts),
        out_shape=jax.ShapeDtypeStruct((N_Z, 24, 512), jnp.bfloat16),
        name="message",
    )(ids, probs, *parts)


def own_columns(values, tp_start, share_width):
    return lax.dynamic_slice_in_dim(values, tp_start, share_width, 1)


def shards(
    tokens,
    norm_gain,
    query_weight,
    key_weight,
    value_weight,
    query_gain,
    key_gain,
    lambdas,
    key_cache,
    value_cache,
    lengths,
    head_gain,
    out_weight,
    ffn_gain,
    dense_gate_weight,
    dense_up_weight,
    dense_down_weight,
    branch_gate,
    expert_ids,
    expert_probs,
    expert_gate,
    expert_up,
    expert_down,
):
    width = tokens.shape[1]
    share_width = width // N_TP
    tp_index = lax.axis_index("tp")
    tp_start = tp_index * share_width
    block = width // N_XC

    select, combine_weights = route_tables(expert_ids, expert_probs)
    message = build_message(
        expert_ids.T,
        expert_probs.T,
        query_weight,
        key_weight,
        value_weight,
        out_weight.T,
        dense_gate_weight,
        dense_up_weight,
        dense_down_weight.T,
    )
    with jax.named_scope("hold"):
        held = exchange(message, Z)
    with jax.named_scope("halves"):
        extra = lax.all_gather(held[:, 16:, :384], "zp", axis=1).reshape(N_Z * 16, 384)
    held = held[:, :16].reshape(N_Z * 16, 512)

    residual = to_mixed(tokens).astype(jnp.float32)
    normed = mixed_scale(residual, to_mixed(norm_gain[None])).astype(jnp.bfloat16)
    xc_index = lax.axis_index(XC)
    with jax.named_scope("spread"):
        spread = lax.all_gather(normed, XC, axis=0)
        spread = lax.dynamic_index_in_dim(spread, xc_index, 1, False).reshape(N_XC * SEQ, block)

    partial_rows = jnp.dot(spread, held, preferred_element_type=jnp.float32)
    with jax.named_scope("project"):
        packed = jnp.sum(exchange(partial_rows.reshape(N_XC, SEQ, 512), XC), axis=0)
    head_out = attend(
        packed, key_cache, value_cache, lengths, query_gain, key_gain, lambdas, head_gain
    )
    with jax.named_scope("heads"):
        all_heads = gather_small(head_out, XC, N_XC).reshape(N_XC * SEQ, 256)
    attended_part = lax.dot_general(
        all_heads, extra[:, :256], (((1,), (1,)), ((), ())), preferred_element_type=jnp.float32
    ).astype(jnp.bfloat16)
    with jax.named_scope("attended"):
        parts = exchange(
            jnp.broadcast_to(
                attended_part.reshape(N_XC, 1, SEQ, block), (N_XC, N_TP, SEQ, block)
            ).reshape(N_XC * N_TP, SEQ, block),
            XC + ("tp",),
        ).reshape(N_XC, N_TP, SEQ, block)
    attended = jnp.sum(parts.astype(jnp.float32), axis=1)
    middle_mixed = lax.optimization_barrier((residual + attended).astype(jnp.bfloat16))
    ffn_input = from_mixed(
        mixed_scale(middle_mixed.astype(jnp.float32), to_mixed(ffn_gain[None])).astype(jnp.bfloat16)
    )
    middle = from_mixed(middle_mixed).astype(jnp.float32)

    ffn_share = own_columns(ffn_input, tp_start, share_width)
    chosen = jnp.dot(
        select.astype(jnp.bfloat16).T, ffn_share, preferred_element_type=jnp.float32
    ).astype(jnp.bfloat16)
    outgoing = jnp.broadcast_to(
        chosen.reshape(1, EXPERTS, CAP, share_width), (REP, EXPERTS, CAP, share_width)
    ).reshape(N_EP, CAP, share_width)
    with jax.named_scope("route"):
        incoming = exchange(outgoing, EP).reshape(N_EP * CAP, share_width)

    with jax.named_scope("dense"):
        dense_held = lax.all_gather(extra[:, 256:], XC, axis=0).reshape(N_XC, N_Z, 16, 128)
    incoming, dense_held = lax.optimization_barrier((incoming, dense_held))
    tag = lax.dynamic_slice_in_dim(dense_held, 2 * xc_index, CAP, 2)[..., 96:100]
    tag = jnp.where(lax.axis_index("zp") == 0, tag[..., :2], tag[..., 2:])
    tag = jnp.sum(tag.transpose(1, 0, 2, 3).reshape(N_EP * CAP, 2).astype(jnp.float32), axis=1)
    dense_held = dense_held.transpose(1, 0, 2, 3).reshape(width, 128)
    down = jnp.concatenate((expert_down[0], dense_held[:, 64:96].T), axis=0)
    dense_held = dense_held[:, :64]

    with jax.named_scope("join"):
        rows = gather_small(incoming, "tp", N_TP)
    rows, dense_held, down, tag = lax.optimization_barrier((rows, dense_held, down, tag))
    rows = rows.transpose(1, 0, 2).reshape(N_EP * CAP, width)
    branch_weight = jax.nn.sigmoid(jnp.sum(rows.astype(jnp.float32) * branch_gate, axis=1))
    dense_scale = branch_weight * tag

    def units(weight):
        return lax.dot_general(
            weight, rows, (((0,), (1,)), ((), ())), preferred_element_type=jnp.float32
        )

    hidden = (jax.nn.silu(units(expert_gate[0])) * units(expert_up[0])).astype(jnp.bfloat16)
    dense_both = units(dense_held)
    dense_hidden = (
        jax.nn.silu(dense_both[:32]) * dense_both[32:] * dense_scale[None]
    ).astype(jnp.bfloat16)
    all_hidden = jnp.concatenate((hidden, dense_hidden), axis=0)
    parts = lax.dot_general(
        all_hidden, down, (((0,), (0,)), ((), ())), preferred_element_type=jnp.float32
    ).astype(jnp.bfloat16)
    parts = parts.reshape(N_EP * CAP, N_TP, share_width).transpose(1, 0, 2)
    with jax.named_scope("reduce"):
        block_out = jnp.sum(exchange(parts, "tp").astype(jnp.float32), axis=0)
    block_out = block_out.astype(jnp.bfloat16).reshape(N_EP, CAP, share_width)
    with jax.named_scope("return"):
        returned = exchange(block_out, EP)
    expert_out = jnp.sum(
        returned.reshape(REP, EXPERTS * CAP, share_width).astype(jnp.float32), axis=0
    )
    routed = jnp.dot(combine_weights, expert_out, precision=lax.Precision.HIGHEST)
    return (own_columns(middle, tp_start, share_width) + routed).astype(jnp.bfloat16)


def solution(mesh):
    fine = Mesh(mesh.devices.reshape(8, 2, 4, 2, 4), ("b", "zp", "x", "c", "tp"))
    return jax.shard_map(
        shards,
        mesh=fine,
        in_specs=(
            P(EP, None),
            P(),
            P(EP, "tp"),
            P(EP, "tp"),
            P(EP, "tp"),
            P(),
            P(),
            P("tp"),
            P(EP, "tp", None, None),
            P(EP, "tp", None, None),
            P(EP),
            P(),
            P("tp", EP),
            P(),
            P(EP, "tp"),
            P(EP, "tp"),
            P("tp", EP),
            P(),
            P(EP, None),
            P(EP, None),
            P(EP, None, "tp"),
            P(EP, None, "tp"),
            P(EP, "tp", None),
        ),
        out_specs=P(EP, "tp"),
        check_vma=False,
    )
```

```python
import jax
import jax.numpy as jnp
from jax import lax
from jax.experimental import pallas as pl
from jax.experimental.pallas import tpu as pltpu
from jax.sharding import Mesh, PartitionSpec as P

SUB = 64
VD = 128
EXPERTS = 16
TOP = 2
CAP = 2


REP = 8
N_Z = 16
N_XC = 8
N_EP = 128
N_TP = 4
SEQ = 8
EP = ("b", "zp", "x", "c")
Z = ("b", "zp")
XC = ("x", "c")

epsilon = 1e-06


def rms_scale(values, scaling):
    return values * lax.rsqrt(jnp.mean(values * values, axis=-1, keepdims=True) + epsilon) * scaling


def mixed_scale(values, scaling):
    mean = jnp.mean(values * values, axis=(0, 2), keepdims=True)
    return values * lax.rsqrt(mean + epsilon) * scaling


def exchange(values, axes):
    return lax.all_to_all(values, axes, split_axis=0, concat_axis=0, tiled=True)


def gather_small(values, axes, count):
    return exchange(jnp.broadcast_to(values[None], (count,) + values.shape), axes)


def to_mixed(rows):
    count = rows.shape[0]
    return rows.reshape(count, N_Z, N_XC, -1).transpose(2, 0, 1, 3).reshape(N_XC, count, -1)


def from_mixed(rows):
    count = rows.shape[1]
    return rows.reshape(N_XC, count, N_Z, -1).transpose(1, 2, 0, 3).reshape(count, -1)


def attend(packed, key_cache, value_cache, lengths, query_gain, key_gain, lambdas, head_gain):
    seq_here = packed.shape[0]
    kv_here = key_cache.shape[1]
    cache_len = key_cache.shape[2]
    heads_here = lambdas.shape[0]
    per_group = heads_here // kv_here
    query_end = heads_here * 2 * SUB
    key_end = query_end + kv_here * 2 * SUB
    mixed = lax.optimization_barrier(packed.astype(jnp.bfloat16))
    query_parts = rms_scale(
        mixed[:, :query_end].astype(jnp.float32).reshape(seq_here, kv_here, per_group, 2, SUB),
        query_gain,
    ).astype(jnp.bfloat16)
    key_parts = rms_scale(
        mixed[:, query_end:key_end].astype(jnp.float32).reshape(seq_here, kv_here, 2, SUB), key_gain
    ).astype(jnp.bfloat16)
    new_values = mixed[:, key_end:].reshape(seq_here, kv_here, VD)
    cached = rms_scale(
        key_cache.astype(jnp.float32).reshape(seq_here, kv_here, cache_len, 2, SUB), key_gain
    ).astype(jnp.bfloat16)
    score_scale = SUB ** (-0.5)
    scores = (
        jnp.einsum("sgqcd,sgjcd->sgqcj", query_parts, cached, preferred_element_type=jnp.float32)
        * score_scale
    )
    own_score = (
        jnp.einsum("sgqcd,sgcd->sgqc", query_parts, key_parts, preferred_element_type=jnp.float32)
        * score_scale
    )
    live_mask = lax.broadcasted_iota(jnp.int32, (seq_here, cache_len), 1) < lengths[:, None]
    exponent = jnp.where(live_mask[:, None, None, None, :], jnp.exp(scores), 0.0)
    own_exponent = jnp.exp(own_score)
    denominator = jnp.sum(exponent, axis=4) + own_exponent
    shares = exponent / denominator[..., None]
    own_shares = own_exponent / denominator
    lam_heads = lambdas.reshape(1, kv_here, per_group)
    mixing = (shares[:, :, :, 0] - lam_heads[..., None] * shares[:, :, :, 1]).astype(jnp.bfloat16)
    own_mixing = lax.optimization_barrier(
        (own_shares[:, :, :, 0] - lam_heads * own_shares[:, :, :, 1]).astype(jnp.bfloat16)
    )
    head_out = jnp.einsum(
        "sgqj,sgje->sgqe", mixing, value_cache, preferred_element_type=jnp.float32
    )
    head_out = (
        head_out
        + own_mixing.astype(jnp.float32)[..., None] * new_values.astype(jnp.float32)[:, :, None, :]
    )
    return rms_scale(head_out, head_gain).astype(jnp.bfloat16).reshape(seq_here, heads_here * VD)


def route_tables(expert_ids, expert_probs):
    seq_here = expert_ids.shape[0]
    paired = expert_ids.reshape(-1)
    total_pairs = paired.shape[0]
    onehot = (paired[:, None] == lax.broadcasted_iota(jnp.int32, (total_pairs, EXPERTS), 1)).astype(
        jnp.float32
    )
    earlier = (
        lax.broadcasted_iota(jnp.int32, (total_pairs, total_pairs), 1)
        < lax.broadcasted_iota(jnp.int32, (total_pairs, total_pairs), 0)
    ).astype(jnp.float32)
    before = jnp.dot(earlier, onehot, precision=lax.Precision.HIGHEST)
    slot_ranks = jnp.sum(before * onehot, axis=1).astype(jnp.int32)
    slot_codes = (paired * CAP + slot_ranks).reshape(seq_here, TOP)
    slots_iota = lax.broadcasted_iota(jnp.int32, (seq_here, TOP, EXPERTS * CAP), 2)
    picked = (slot_codes[:, :, None] == slots_iota).astype(jnp.float32)
    select = jnp.sum(picked, axis=1)
    combine_weights = jnp.sum(picked * expert_probs[:, :, None], axis=1)
    return (select, combine_weights)


def message_body(ids, probs, query, key, value, out, gate, up, down, message):
    lanes = lax.broadcasted_iota(jnp.int32, (16, 256), 1)
    narrow = lax.broadcasted_iota(jnp.int32, (16, 128), 1)
    places = lax.broadcasted_iota(jnp.int32, (16, 128), 0)
    shared = jnp.concatenate((query[...], key[...], value[...]), axis=1)
    wide = [part[...].astype(jnp.float32) for part in (gate, up, down)]
    held = out[...].astype(jnp.float32)
    tags = [jnp.zeros((16, 128), jnp.float32) for _ in range(2)]
    for row in range(SEQ):
        chosen = ids[0, row]
        rank = jnp.int32(0)
        for earlier in range(row):
            for choice in range(TOP):
                rank = rank + (ids[choice, earlier] == chosen).astype(jnp.int32)
        slot = chosen * CAP + rank
        for half in range(2):
            tags[half] = jnp.where(places + 16 * half == slot, probs[0, row], tags[half])
    tagged = jnp.zeros((16, 128), jnp.float32)
    for half in range(2):
        used = tags[half] > 0.0
        inverse = jnp.where(used, 1.0 / jnp.where(used, tags[half], 1.0), 0.0)
        high = inverse.astype(jnp.bfloat16).astype(jnp.float32)
        tagged = jnp.where(narrow == 96 + 2 * half, high, tagged)
        tagged = jnp.where(narrow == 97 + 2 * half, inverse - high, tagged)
    for rep in range(REP):
        turned = [
            pltpu.roll(part, (32 * (place - rep)) % 256, 1) for place, part in enumerate(wide)
        ]
        own = jnp.where(
            lanes < 32, turned[0], jnp.where(lanes < 64, turned[1], turned[2])
        )[:, :128]
        own = jnp.where(narrow < 96, own, tagged)
        extra = jnp.concatenate((held, own, jnp.zeros((16, 128), jnp.float32)), axis=1)
        for half in range(2):
            message[2 * rep + half, :16, :] = shared
            message[2 * rep + half, 16:, :] = extra[8 * half : 8 * half + 8].astype(jnp.bfloat16)


def build_message(ids, probs, *parts):
    scalars = pl.BlockSpec(memory_space=pltpu.SMEM)
    whole = pl.BlockSpec(memory_space=pltpu.VMEM)
    return pl.pallas_call(
        message_body,
        in_specs=[scalars, scalars] + [whole] * len(parts),
        out_shape=jax.ShapeDtypeStruct((N_Z, 24, 512), jnp.bfloat16),
        name="message",
    )(ids, probs, *parts)


def own_columns(values, tp_start, share_width):
    return lax.dynamic_slice_in_dim(values, tp_start, share_width, 1)


def shards(
    tokens,
    norm_gain,
    query_weight,
    key_weight,
    value_weight,
    query_gain,
    key_gain,
    lambdas,
    key_cache,
    value_cache,
    lengths,
    head_gain,
    out_weight,
    ffn_gain,
    dense_gate_weight,
    dense_up_weight,
    dense_down_weight,
    branch_gate,
    expert_ids,
    expert_probs,
    expert_gate,
    expert_up,
    expert_down,
):
    width = tokens.shape[1]
    share_width = width // N_TP
    tp_index = lax.axis_index("tp")
    tp_start = (tp_index * share_width).astype(jnp.uint32)
    block = width // N_XC

    select, combine_weights = route_tables(expert_ids, expert_probs)
    message = build_message(
        expert_ids.T,
        expert_probs.T,
        query_weight,
        key_weight,
        value_weight,
        out_weight.T,
        dense_gate_weight,
        dense_up_weight,
        dense_down_weight.T,
    )
    with jax.named_scope("hold"):
        held = exchange(message, Z)
    with jax.named_scope("halves"):
        extra = lax.all_gather(held[:, 16:, :384], "zp", axis=1).reshape(N_Z * 16, 384)
    residual = to_mixed(tokens).astype(jnp.float32)
    normed = mixed_scale(residual, to_mixed(norm_gain[None])).astype(jnp.bfloat16)
    xc_index = lax.axis_index(XC)
    with jax.named_scope("spread"):
        spread = lax.all_gather(normed, XC, axis=0)
        spread = lax.dynamic_index_in_dim(spread, xc_index, 1, False).reshape(N_XC * SEQ, block)

    held, select, combine_weights, ffn_scaling, residual = lax.optimization_barrier(
        (
            held[:, :16].reshape(N_Z * 16, 512),
            select.astype(jnp.bfloat16).T,
            combine_weights,
            to_mixed(ffn_gain[None]),
            residual,
        )
    )
    partial_rows = jnp.dot(spread, held, preferred_element_type=jnp.float32)
    with jax.named_scope("project"):
        packed = exchange(partial_rows.reshape(N_XC, SEQ, 512), XC)
        packed, extra = lax.optimization_barrier((packed, extra))
        packed = jnp.sum(packed, axis=0)
    head_out = attend(
        packed, key_cache, value_cache, lengths, query_gain, key_gain, lambdas, head_gain
    )
    head_out, tp_start = lax.optimization_barrier((head_out, tp_start))
    with jax.named_scope("heads"):
        all_heads = gather_small(head_out, XC, N_XC).reshape(N_XC * SEQ, 256)
    attended_part = lax.dot_general(
        all_heads, extra[:, :256], (((1,), (1,)), ((), ())), preferred_element_type=jnp.float32
    ).astype(jnp.bfloat16)
    with jax.named_scope("attended"):
        parts = exchange(
            jnp.broadcast_to(
                attended_part.reshape(N_XC, 1, SEQ, block), (N_XC, N_TP, SEQ, block)
            ).reshape(N_XC * N_TP, SEQ, block),
            XC + ("tp",),
        ).reshape(N_XC, N_TP, SEQ, block)
    attended = jnp.sum(parts.astype(jnp.float32), axis=1)
    middle_mixed = lax.optimization_barrier((residual + attended).astype(jnp.bfloat16))
    ffn_input = from_mixed(
        mixed_scale(middle_mixed.astype(jnp.float32), ffn_scaling).astype(jnp.bfloat16)
    )
    middle = own_columns(from_mixed(middle_mixed).astype(jnp.float32), tp_start, share_width)

    ffn_share = own_columns(ffn_input, tp_start, share_width)
    chosen = jnp.dot(
        select, ffn_share, preferred_element_type=jnp.float32
    ).astype(jnp.bfloat16)
    outgoing = jnp.broadcast_to(
        chosen.reshape(1, EXPERTS, CAP, share_width), (REP, EXPERTS, CAP, share_width)
    ).reshape(N_EP, CAP, share_width)
    with jax.named_scope("route"):
        incoming = exchange(outgoing, EP).reshape(N_EP * CAP, share_width)

    with jax.named_scope("dense"):
        dense_held = lax.all_gather(extra[:, 256:], XC, axis=0).reshape(N_XC, N_Z, 16, 128)
    incoming, dense_held = lax.optimization_barrier((incoming, dense_held))
    tag = lax.dynamic_slice_in_dim(dense_held, 2 * xc_index, CAP, 2)[..., 96:100]
    tag = jnp.where(lax.axis_index("zp") == 0, tag[..., :2], tag[..., 2:])
    tag = jnp.sum(tag.transpose(1, 0, 2, 3).reshape(N_EP * CAP, 2).astype(jnp.float32), axis=1)
    dense_held = dense_held.transpose(1, 0, 2, 3).reshape(width, 128)
    down = jnp.concatenate((expert_down[0], dense_held[:, 64:96].T), axis=0)
    dense_held = dense_held[:, :64]

    with jax.named_scope("join"):
        rows = gather_small(incoming, "tp", N_TP)
    rows, dense_held, down, tag, middle, combine_weights = lax.optimization_barrier(
        (rows, dense_held, down, tag, middle, combine_weights)
    )
    rows = rows.transpose(1, 0, 2).reshape(N_EP * CAP, width)
    branch_weight = jax.nn.sigmoid(jnp.sum(rows.astype(jnp.float32) * branch_gate, axis=1))
    dense_scale = branch_weight * tag

    def units(weight):
        return lax.dot_general(
            weight, rows, (((0,), (1,)), ((), ())), preferred_element_type=jnp.float32
        )

    hidden = (jax.nn.silu(units(expert_gate[0])) * units(expert_up[0])).astype(jnp.bfloat16)
    dense_both = units(dense_held)
    dense_hidden = (
        jax.nn.silu(dense_both[:32]) * dense_both[32:] * dense_scale[None]
    ).astype(jnp.bfloat16)
    all_hidden = jnp.concatenate((hidden, dense_hidden), axis=0)
    parts = lax.dot_general(
        all_hidden, down, (((0,), (0,)), ((), ())), preferred_element_type=jnp.float32
    ).astype(jnp.bfloat16)
    parts = parts.reshape(N_EP * CAP, N_TP, share_width).transpose(1, 0, 2)
    with jax.named_scope("reduce"):
        block_out = jnp.sum(exchange(parts, "tp").astype(jnp.float32), axis=0)
    block_out = block_out.astype(jnp.bfloat16).reshape(N_EP, CAP, share_width)
    with jax.named_scope("return"):
        returned = exchange(block_out, EP)
    expert_out = jnp.sum(
        returned.reshape(REP, EXPERTS * CAP, share_width).astype(jnp.float32), axis=0
    )
    routed = jnp.dot(combine_weights, expert_out, precision=lax.Precision.HIGHEST)
    return (middle + routed).astype(jnp.bfloat16)


def solution(mesh):
    fine = Mesh(mesh.devices.reshape(8, 2, 4, 2, 4), ("b", "zp", "x", "c", "tp"))
    return jax.shard_map(
        shards,
        mesh=fine,
        in_specs=(
            P(EP, None),
            P(),
            P(EP, "tp"),
            P(EP, "tp"),
            P(EP, "tp"),
            P(),
            P(),
            P("tp"),
            P(EP, "tp", None, None),
            P(EP, "tp", None, None),
            P(EP),
            P(),
            P("tp", EP),
            P(),
            P(EP, "tp"),
            P(EP, "tp"),
            P("tp", EP),
            P(),
            P(EP, None),
            P(EP, None),
            P(EP, None, "tp"),
            P(EP, None, "tp"),
            P(EP, "tp", None),
        ),
        out_specs=P(EP, "tp"),
        check_vma=False,
    )
```

```python
import jax
import jax.numpy as jnp
from jax import lax
from jax.experimental import pallas as pl
from jax.experimental.pallas import tpu as pltpu
from jax.sharding import Mesh, PartitionSpec as P

SUB = 64
VD = 128
EXPERTS = 16
TOP = 2
CAP = 2


REP = 8
N_Z = 16
N_XC = 8
N_EP = 128
N_TP = 4
SEQ = 8
EP = ("b", "zp", "x", "c")
Z = ("b", "zp")
XC = ("x", "c")

epsilon = 1e-06


def rms_scale(values, scaling):
    return values * lax.rsqrt(jnp.mean(values * values, axis=-1, keepdims=True) + epsilon) * scaling


def mixed_scale(values, scaling):
    mean = jnp.mean(values * values, axis=(0, 2), keepdims=True)
    return values * lax.rsqrt(mean + epsilon) * scaling


def exchange(values, axes):
    return lax.all_to_all(values, axes, split_axis=0, concat_axis=0, tiled=True)


def gather_small(values, axes, count):
    return exchange(jnp.broadcast_to(values[None], (count,) + values.shape), axes)


def to_mixed(rows):
    count = rows.shape[0]
    return rows.reshape(count, N_Z, N_XC, -1).transpose(2, 0, 1, 3).reshape(N_XC, count, -1)


def from_mixed(rows):
    count = rows.shape[1]
    return rows.reshape(N_XC, count, N_Z, -1).transpose(1, 2, 0, 3).reshape(count, -1)


def attend(packed, key_cache, value_cache, lengths, query_gain, key_gain, lambdas, head_gain):
    seq_here = packed.shape[0]
    kv_here = key_cache.shape[1]
    cache_len = key_cache.shape[2]
    heads_here = lambdas.shape[0]
    per_group = heads_here // kv_here
    query_end = heads_here * 2 * SUB
    key_end = query_end + kv_here * 2 * SUB
    mixed = lax.optimization_barrier(packed.astype(jnp.bfloat16))
    query_parts = rms_scale(
        mixed[:, :query_end].astype(jnp.float32).reshape(seq_here, kv_here, per_group, 2, SUB),
        query_gain,
    ).astype(jnp.bfloat16)
    key_parts = rms_scale(
        mixed[:, query_end:key_end].astype(jnp.float32).reshape(seq_here, kv_here, 2, SUB), key_gain
    ).astype(jnp.bfloat16)
    new_values = mixed[:, key_end:].reshape(seq_here, kv_here, VD)
    cached = rms_scale(
        key_cache.astype(jnp.float32).reshape(seq_here, kv_here, cache_len, 2, SUB), key_gain
    ).astype(jnp.bfloat16)
    score_scale = SUB ** (-0.5)
    scores = (
        jnp.einsum("sgqcd,sgjcd->sgqcj", query_parts, cached, preferred_element_type=jnp.float32)
        * score_scale
    )
    own_score = (
        jnp.einsum("sgqcd,sgcd->sgqc", query_parts, key_parts, preferred_element_type=jnp.float32)
        * score_scale
    )
    live_mask = lax.broadcasted_iota(jnp.int32, (seq_here, cache_len), 1) < lengths[:, None]
    exponent = jnp.where(live_mask[:, None, None, None, :], jnp.exp(scores), 0.0)
    own_exponent = jnp.exp(own_score)
    denominator = jnp.sum(exponent, axis=4) + own_exponent
    shares = exponent / denominator[..., None]
    own_shares = own_exponent / denominator
    lam_heads = lambdas.reshape(1, kv_here, per_group)
    mixing = (shares[:, :, :, 0] - lam_heads[..., None] * shares[:, :, :, 1]).astype(jnp.bfloat16)
    own_mixing = lax.optimization_barrier(
        (own_shares[:, :, :, 0] - lam_heads * own_shares[:, :, :, 1]).astype(jnp.bfloat16)
    )
    head_out = jnp.einsum(
        "sgqj,sgje->sgqe", mixing, value_cache, preferred_element_type=jnp.float32
    )
    head_out = (
        head_out
        + own_mixing.astype(jnp.float32)[..., None] * new_values.astype(jnp.float32)[:, :, None, :]
    )
    return rms_scale(head_out, head_gain).astype(jnp.bfloat16).reshape(seq_here, heads_here * VD)


def route_tables(expert_ids, expert_probs):
    seq_here = expert_ids.shape[0]
    paired = expert_ids.reshape(-1)
    total_pairs = paired.shape[0]
    onehot = (paired[:, None] == lax.broadcasted_iota(jnp.int32, (total_pairs, EXPERTS), 1)).astype(
        jnp.float32
    )
    earlier = (
        lax.broadcasted_iota(jnp.int32, (total_pairs, total_pairs), 1)
        < lax.broadcasted_iota(jnp.int32, (total_pairs, total_pairs), 0)
    ).astype(jnp.float32)
    before = jnp.dot(earlier, onehot, precision=lax.Precision.HIGHEST)
    slot_ranks = jnp.sum(before * onehot, axis=1).astype(jnp.int32)
    slot_codes = (paired * CAP + slot_ranks).reshape(seq_here, TOP)
    slots_iota = lax.broadcasted_iota(jnp.int32, (seq_here, TOP, EXPERTS * CAP), 2)
    picked = (slot_codes[:, :, None] == slots_iota).astype(jnp.float32)
    select = jnp.sum(picked, axis=1)
    combine_weights = jnp.sum(picked * expert_probs[:, :, None], axis=1)
    return (select, combine_weights)


def message_body(ids, probs, query, key, value, out, gate, up, down, message):
    lanes = lax.broadcasted_iota(jnp.int32, (16, 256), 1)
    narrow = lax.broadcasted_iota(jnp.int32, (16, 128), 1)
    places = lax.broadcasted_iota(jnp.int32, (16, 128), 0)
    shared = jnp.concatenate((query[...], key[...], value[...]), axis=1)
    wide = [part[...].astype(jnp.float32) for part in (gate, up, down)]
    held = out[...].astype(jnp.float32)
    tags = [jnp.zeros((16, 128), jnp.float32) for _ in range(2)]
    for row in range(SEQ):
        chosen = ids[0, row]
        rank = jnp.int32(0)
        for earlier in range(row):
            for choice in range(TOP):
                rank = rank + (ids[choice, earlier] == chosen).astype(jnp.int32)
        slot = chosen * CAP + rank
        for half in range(2):
            tags[half] = jnp.where(places + 16 * half == slot, probs[0, row], tags[half])
    tagged = jnp.zeros((16, 128), jnp.float32)
    for half in range(2):
        used = tags[half] > 0.0
        inverse = jnp.where(used, 1.0 / jnp.where(used, tags[half], 1.0), 0.0)
        high = inverse.astype(jnp.bfloat16).astype(jnp.float32)
        tagged = jnp.where(narrow == 96 + 2 * half, high, tagged)
        tagged = jnp.where(narrow == 97 + 2 * half, inverse - high, tagged)
    for rep in range(REP):
        turned = [
            pltpu.roll(part, (32 * (place - rep)) % 256, 1) for place, part in enumerate(wide)
        ]
        own = jnp.where(
            lanes < 32, turned[0], jnp.where(lanes < 64, turned[1], turned[2])
        )[:, :128]
        own = jnp.where(narrow < 96, own, tagged)
        extra = jnp.concatenate((held, own, jnp.zeros((16, 128), jnp.float32)), axis=1)
        for half in range(2):
            message[2 * rep + half, :16, :] = shared
            message[2 * rep + half, 16:, :] = extra[8 * half : 8 * half + 8].astype(jnp.bfloat16)


def build_message(ids, probs, *parts):
    scalars = pl.BlockSpec(memory_space=pltpu.SMEM)
    whole = pl.BlockSpec(memory_space=pltpu.VMEM)
    return pl.pallas_call(
        message_body,
        in_specs=[scalars, scalars] + [whole] * len(parts),
        out_shape=jax.ShapeDtypeStruct((N_Z, 24, 512), jnp.bfloat16),
        name="message",
    )(ids, probs, *parts)


def own_columns(values, tp_start, share_width):
    return lax.dynamic_slice_in_dim(values, tp_start, share_width, 1)


def shards(
    tokens,
    norm_gain,
    query_weight,
    key_weight,
    value_weight,
    query_gain,
    key_gain,
    lambdas,
    key_cache,
    value_cache,
    lengths,
    head_gain,
    out_weight,
    ffn_gain,
    dense_gate_weight,
    dense_up_weight,
    dense_down_weight,
    branch_gate,
    expert_ids,
    expert_probs,
    expert_gate,
    expert_up,
    expert_down,
):
    width = tokens.shape[1]
    share_width = width // N_TP
    tp_index = lax.axis_index("tp")
    tp_start = (tp_index * share_width).astype(jnp.uint32)
    block = width // N_XC

    select, combine_weights = route_tables(expert_ids, expert_probs)
    message = build_message(
        expert_ids.T,
        expert_probs.T,
        query_weight,
        key_weight,
        value_weight,
        out_weight.T,
        dense_gate_weight,
        dense_up_weight,
        dense_down_weight.T,
    )
    with jax.named_scope("hold"):
        held = exchange(message, Z)
    with jax.named_scope("halves"):
        extra = lax.all_gather(held[:, 16:, :384], "zp", axis=1).reshape(N_Z * 16, 384)
    residual = to_mixed(tokens).astype(jnp.float32)
    normed = mixed_scale(residual, to_mixed(norm_gain[None])).astype(jnp.bfloat16)
    xc_index = lax.axis_index(XC)
    with jax.named_scope("spread"):
        spread = lax.all_gather(normed, XC, axis=0)
        spread = lax.dynamic_index_in_dim(spread, xc_index, 1, False).reshape(N_XC * SEQ, block)

    held, select, combine_weights, ffn_scaling, residual = lax.optimization_barrier(
        (
            held[:, :16].reshape(N_Z * 16, 512),
            select.astype(jnp.bfloat16).T,
            combine_weights,
            to_mixed(ffn_gain[None]),
            residual,
        )
    )
    partial_rows = jnp.dot(spread, held, preferred_element_type=jnp.float32)
    partial_rows, key_cache = lax.optimization_barrier((partial_rows, key_cache))
    with jax.named_scope("project"):
        packed = exchange(partial_rows.reshape(N_XC, SEQ, 512), XC)
        packed = jnp.sum(packed, axis=0)
    head_out = attend(
        packed, key_cache, value_cache, lengths, query_gain, key_gain, lambdas, head_gain
    )
    head_out, tp_start = lax.optimization_barrier((head_out, tp_start))
    with jax.named_scope("heads"):
        all_heads = gather_small(head_out, XC, N_XC).reshape(N_XC * SEQ, 256)
    all_heads, extra = lax.optimization_barrier((all_heads, extra))
    attended_part = lax.dot_general(
        all_heads, extra[:, :256], (((1,), (1,)), ((), ())), preferred_element_type=jnp.float32
    ).astype(jnp.bfloat16)
    with jax.named_scope("attended"):
        parts = exchange(
            jnp.broadcast_to(
                attended_part.reshape(N_XC, 1, SEQ, block), (N_XC, N_TP, SEQ, block)
            ).reshape(N_XC * N_TP, SEQ, block),
            XC + ("tp",),
        ).reshape(N_XC, N_TP, SEQ, block)
    attended = jnp.sum(parts.astype(jnp.float32), axis=1)
    middle_mixed = lax.optimization_barrier((residual + attended).astype(jnp.bfloat16))
    ffn_input = from_mixed(
        mixed_scale(middle_mixed.astype(jnp.float32), ffn_scaling).astype(jnp.bfloat16)
    )
    middle = own_columns(from_mixed(middle_mixed).astype(jnp.float32), tp_start, share_width)

    ffn_share = own_columns(ffn_input, tp_start, share_width)
    chosen = jnp.dot(
        select, ffn_share, preferred_element_type=jnp.float32
    ).astype(jnp.bfloat16)
    outgoing = jnp.broadcast_to(
        chosen.reshape(1, EXPERTS, CAP, share_width), (REP, EXPERTS, CAP, share_width)
    ).reshape(N_EP, CAP, share_width)
    with jax.named_scope("route"):
        incoming = exchange(outgoing, EP).reshape(N_EP * CAP, share_width)

    with jax.named_scope("dense"):
        dense_held = lax.all_gather(extra[:, 256:], XC, axis=0).reshape(N_XC, N_Z, 16, 128)
    incoming, dense_held = lax.optimization_barrier((incoming, dense_held))
    tag = lax.dynamic_slice_in_dim(dense_held, 2 * xc_index, CAP, 2)[..., 96:100]
    tag = jnp.where(lax.axis_index("zp") == 0, tag[..., :2], tag[..., 2:])
    tag = jnp.sum(tag.transpose(1, 0, 2, 3).reshape(N_EP * CAP, 2).astype(jnp.float32), axis=1)
    dense_held = dense_held.transpose(1, 0, 2, 3).reshape(width, 128)
    down = jnp.concatenate((expert_down[0], dense_held[:, 64:96].T), axis=0)
    dense_held = dense_held[:, :64]

    with jax.named_scope("join"):
        rows = gather_small(incoming, "tp", N_TP)
    rows, dense_held, down, tag, middle, combine_weights = lax.optimization_barrier(
        (rows, dense_held, down, tag, middle, combine_weights)
    )
    rows = rows.transpose(1, 0, 2).reshape(N_EP * CAP, width)
    branch_weight = jax.nn.sigmoid(jnp.sum(rows.astype(jnp.float32) * branch_gate, axis=1))
    dense_scale = branch_weight * tag

    def units(weight):
        return lax.dot_general(
            weight, rows, (((0,), (1,)), ((), ())), preferred_element_type=jnp.float32
        )

    hidden = (jax.nn.silu(units(expert_gate[0])) * units(expert_up[0])).astype(jnp.bfloat16)
    dense_both = units(dense_held)
    dense_hidden = (
        jax.nn.silu(dense_both[:32]) * dense_both[32:] * dense_scale[None]
    ).astype(jnp.bfloat16)
    all_hidden = jnp.concatenate((hidden, dense_hidden), axis=0)
    parts = lax.dot_general(
        all_hidden, down, (((0,), (0,)), ((), ())), preferred_element_type=jnp.float32
    ).astype(jnp.bfloat16)
    parts = parts.reshape(N_EP * CAP, N_TP, share_width).transpose(1, 0, 2)
    with jax.named_scope("reduce"):
        block_out = jnp.sum(exchange(parts, "tp").astype(jnp.float32), axis=0)
    block_out = block_out.astype(jnp.bfloat16).reshape(N_EP, CAP, share_width)
    with jax.named_scope("return"):
        returned = exchange(block_out, EP)
    expert_out = jnp.sum(
        returned.reshape(REP, EXPERTS * CAP, share_width).astype(jnp.float32), axis=0
    )
    routed = jnp.dot(combine_weights, expert_out, precision=lax.Precision.HIGHEST)
    return (middle + routed).astype(jnp.bfloat16)


def solution(mesh):
    fine = Mesh(mesh.devices.reshape(8, 2, 4, 2, 4), ("b", "zp", "x", "c", "tp"))
    return jax.shard_map(
        shards,
        mesh=fine,
        in_specs=(
            P(EP, None),
            P(),
            P(EP, "tp"),
            P(EP, "tp"),
            P(EP, "tp"),
            P(),
            P(),
            P("tp"),
            P(EP, "tp", None, None),
            P(EP, "tp", None, None),
            P(EP),
            P(),
            P("tp", EP),
            P(),
            P(EP, "tp"),
            P(EP, "tp"),
            P("tp", EP),
            P(),
            P(EP, None),
            P(EP, None),
            P(EP, None, "tp"),
            P(EP, None, "tp"),
            P(EP, "tp", None),
        ),
        out_specs=P(EP, "tp"),
        check_vma=False,
    )
```

```python
import jax
import jax.numpy as jnp
from jax import lax
from jax.experimental import pallas as pl
from jax.experimental.pallas import tpu as pltpu
from jax.sharding import Mesh, PartitionSpec as P

SUB = 64
VD = 128
EXPERTS = 16
TOP = 2
CAP = 2


REP = 8
N_Z = 16
N_XC = 8
N_EP = 128
N_TP = 4
SEQ = 8
EP = ("b", "zp", "x", "c")
Z = ("b", "zp")
XC = ("x", "c")

epsilon = 1e-06


def rms_scale(values, scaling):
    return values * lax.rsqrt(jnp.mean(values * values, axis=-1, keepdims=True) + epsilon) * scaling


def mixed_scale(values, scaling):
    mean = jnp.mean(values * values, axis=(0, 2), keepdims=True)
    return values * lax.rsqrt(mean + epsilon) * scaling


def exchange(values, axes):
    return lax.all_to_all(values, axes, split_axis=0, concat_axis=0, tiled=True)


def gather_small(values, axes, count):
    return exchange(jnp.broadcast_to(values[None], (count,) + values.shape), axes)


def to_mixed(rows):
    count = rows.shape[0]
    return rows.reshape(count, N_Z, N_XC, -1).transpose(2, 0, 1, 3).reshape(N_XC, count, -1)


def from_mixed(rows):
    count = rows.shape[1]
    return rows.reshape(N_XC, count, N_Z, -1).transpose(1, 2, 0, 3).reshape(count, -1)


def attend(packed, key_cache, value_cache, lengths, query_gain, key_gain, lambdas, head_gain):
    seq_here = packed.shape[0]
    kv_here = key_cache.shape[1]
    cache_len = key_cache.shape[2]
    heads_here = lambdas.shape[0]
    per_group = heads_here // kv_here
    query_end = heads_here * 2 * SUB
    key_end = query_end + kv_here * 2 * SUB
    mixed = lax.optimization_barrier(packed.astype(jnp.bfloat16))
    query_parts = rms_scale(
        mixed[:, :query_end].astype(jnp.float32).reshape(seq_here, kv_here, per_group, 2, SUB),
        query_gain,
    ).astype(jnp.bfloat16)
    key_parts = rms_scale(
        mixed[:, query_end:key_end].astype(jnp.float32).reshape(seq_here, kv_here, 2, SUB), key_gain
    ).astype(jnp.bfloat16)
    new_values = mixed[:, key_end:].reshape(seq_here, kv_here, VD)
    cached = rms_scale(
        key_cache.astype(jnp.float32).reshape(seq_here, kv_here, cache_len, 2, SUB), key_gain
    ).astype(jnp.bfloat16)
    score_scale = SUB ** (-0.5)
    scores = (
        jnp.einsum("sgqcd,sgjcd->sgqcj", query_parts, cached, preferred_element_type=jnp.float32)
        * score_scale
    )
    own_score = (
        jnp.einsum("sgqcd,sgcd->sgqc", query_parts, key_parts, preferred_element_type=jnp.float32)
        * score_scale
    )
    live_mask = lax.broadcasted_iota(jnp.int32, (seq_here, cache_len), 1) < lengths[:, None]
    exponent = jnp.where(live_mask[:, None, None, None, :], jnp.exp(scores), 0.0)
    own_exponent = jnp.exp(own_score)
    denominator = jnp.sum(exponent, axis=4) + own_exponent
    shares = exponent / denominator[..., None]
    own_shares = own_exponent / denominator
    lam_heads = lambdas.reshape(1, kv_here, per_group)
    mixing = (shares[:, :, :, 0] - lam_heads[..., None] * shares[:, :, :, 1]).astype(jnp.bfloat16)
    own_mixing = lax.optimization_barrier(
        (own_shares[:, :, :, 0] - lam_heads * own_shares[:, :, :, 1]).astype(jnp.bfloat16)
    )
    head_out = jnp.einsum(
        "sgqj,sgje->sgqe", mixing, value_cache, preferred_element_type=jnp.float32
    )
    head_out = (
        head_out
        + own_mixing.astype(jnp.float32)[..., None] * new_values.astype(jnp.float32)[:, :, None, :]
    )
    return rms_scale(head_out, head_gain).astype(jnp.bfloat16).reshape(seq_here, heads_here * VD)


def route_tables(expert_ids, expert_probs):
    seq_here = expert_ids.shape[0]
    paired = expert_ids.reshape(-1)
    total_pairs = paired.shape[0]
    onehot = (paired[:, None] == lax.broadcasted_iota(jnp.int32, (total_pairs, EXPERTS), 1)).astype(
        jnp.float32
    )
    earlier = (
        lax.broadcasted_iota(jnp.int32, (total_pairs, total_pairs), 1)
        < lax.broadcasted_iota(jnp.int32, (total_pairs, total_pairs), 0)
    ).astype(jnp.float32)
    before = jnp.dot(earlier, onehot, precision=lax.Precision.HIGHEST)
    slot_ranks = jnp.sum(before * onehot, axis=1).astype(jnp.int32)
    slot_codes = (paired * CAP + slot_ranks).reshape(seq_here, TOP)
    slots_iota = lax.broadcasted_iota(jnp.int32, (seq_here, TOP, EXPERTS * CAP), 2)
    picked = (slot_codes[:, :, None] == slots_iota).astype(jnp.float32)
    select = jnp.sum(picked, axis=1)
    combine_weights = jnp.sum(picked * expert_probs[:, :, None], axis=1)
    return (select, combine_weights)


def message_body(ids, probs, query, key, value, out, gate, up, down, message):
    lanes = lax.broadcasted_iota(jnp.int32, (16, 256), 1)
    narrow = lax.broadcasted_iota(jnp.int32, (16, 128), 1)
    places = lax.broadcasted_iota(jnp.int32, (16, 128), 0)
    shared = jnp.concatenate((query[...], key[...], value[...], out[...]), axis=1)
    wide = [part[...].astype(jnp.float32) for part in (gate, up, down)]
    tags = [jnp.zeros((16, 128), jnp.float32) for _ in range(2)]
    for row in range(SEQ):
        chosen = ids[0, row]
        rank = jnp.int32(0)
        for earlier in range(row):
            for choice in range(TOP):
                rank = rank + (ids[choice, earlier] == chosen).astype(jnp.int32)
        slot = chosen * CAP + rank
        for half in range(2):
            tags[half] = jnp.where(places + 16 * half == slot, probs[0, row], tags[half])
    for half in range(2):
        used = tags[half] > 0.0
        inverse = jnp.where(used, 1.0 / jnp.where(used, tags[half], 1.0), 0.0)
        high = inverse.astype(jnp.bfloat16).astype(jnp.float32)
        tags[half] = jnp.where(
            narrow == 96, high, jnp.where(narrow == 97, inverse - high, 0.0)
        )
    for rep in range(REP):
        turned = [
            pltpu.roll(part, (32 * (place - rep)) % 256, 1) for place, part in enumerate(wide)
        ]
        own = jnp.where(
            lanes < 32, turned[0], jnp.where(lanes < 64, turned[1], turned[2])
        )[:, :128]
        own = jnp.where(narrow < 96, own, 0.0)
        for half in range(2):
            message[2 * rep + half, :, :768] = shared
            message[2 * rep + half, :, 768:] = (own + tags[half]).astype(jnp.bfloat16)


def build_message(ids, probs, *parts):
    scalars = pl.BlockSpec(memory_space=pltpu.SMEM)
    whole = pl.BlockSpec(memory_space=pltpu.VMEM)
    return pl.pallas_call(
        message_body,
        in_specs=[scalars, scalars] + [whole] * len(parts),
        out_shape=jax.ShapeDtypeStruct((N_Z, 16, 896), jnp.bfloat16),
        name="message",
    )(ids, probs, *parts)


def own_columns(values, tp_start, share_width):
    return lax.dynamic_slice_in_dim(values, tp_start, share_width, 1)


def shards(
    tokens,
    norm_gain,
    query_weight,
    key_weight,
    value_weight,
    query_gain,
    key_gain,
    lambdas,
    key_cache,
    value_cache,
    lengths,
    head_gain,
    out_weight,
    ffn_gain,
    dense_gate_weight,
    dense_up_weight,
    dense_down_weight,
    branch_gate,
    expert_ids,
    expert_probs,
    expert_gate,
    expert_up,
    expert_down,
):
    width = tokens.shape[1]
    share_width = width // N_TP
    tp_index = lax.axis_index("tp")
    tp_start = (tp_index * share_width).astype(jnp.uint32)
    block = width // N_XC

    select, combine_weights = route_tables(expert_ids, expert_probs)
    message = build_message(
        expert_ids.T,
        expert_probs.T,
        query_weight,
        key_weight,
        value_weight,
        out_weight.T,
        dense_gate_weight,
        dense_up_weight,
        dense_down_weight.T,
    )
    with jax.named_scope("hold"):
        held = exchange(message, Z)
    held = held.reshape(N_Z * 16, 896)
    held, extra = held[:, :512], held[:, 512:]
    residual = to_mixed(tokens).astype(jnp.float32)
    normed = mixed_scale(residual, to_mixed(norm_gain[None])).astype(jnp.bfloat16)
    xc_index = lax.axis_index(XC)
    with jax.named_scope("spread"):
        spread = lax.all_gather(normed, XC, axis=0)
        spread = lax.dynamic_index_in_dim(spread, xc_index, 1, False).reshape(N_XC * SEQ, block)

    held, select, combine_weights, ffn_scaling, residual = lax.optimization_barrier(
        (
            held,
            select.astype(jnp.bfloat16).T,
            combine_weights,
            to_mixed(ffn_gain[None]),
            residual,
        )
    )
    partial_rows = jnp.dot(spread, held, preferred_element_type=jnp.float32)
    partial_rows, key_cache = lax.optimization_barrier((partial_rows, key_cache))
    with jax.named_scope("project"):
        packed = exchange(partial_rows.reshape(N_XC, SEQ, 512), XC)
        packed = jnp.sum(packed, axis=0)
    head_out = attend(
        packed, key_cache, value_cache, lengths, query_gain, key_gain, lambdas, head_gain
    )
    head_out, tp_start = lax.optimization_barrier((head_out, tp_start))
    with jax.named_scope("heads"):
        all_heads = gather_small(head_out, XC, N_XC).reshape(N_XC * SEQ, 256)
    attended_part = lax.dot_general(
        all_heads, extra[:, :256], (((1,), (1,)), ((), ())), preferred_element_type=jnp.float32
    ).astype(jnp.bfloat16)
    with jax.named_scope("attended"):
        parts = exchange(
            jnp.broadcast_to(
                attended_part.reshape(N_XC, 1, SEQ, block), (N_XC, N_TP, SEQ, block)
            ).reshape(N_XC * N_TP, SEQ, block),
            XC + ("tp",),
        ).reshape(N_XC, N_TP, SEQ, block)
    attended = jnp.sum(parts.astype(jnp.float32), axis=1)
    middle_mixed = lax.optimization_barrier((residual + attended).astype(jnp.bfloat16))
    ffn_input = from_mixed(
        mixed_scale(middle_mixed.astype(jnp.float32), ffn_scaling).astype(jnp.bfloat16)
    )
    middle = own_columns(from_mixed(middle_mixed).astype(jnp.float32), tp_start, share_width)

    ffn_share = own_columns(ffn_input, tp_start, share_width)
    chosen = jnp.dot(
        select, ffn_share, preferred_element_type=jnp.float32
    ).astype(jnp.bfloat16)
    outgoing = jnp.broadcast_to(
        chosen.reshape(1, EXPERTS, CAP, share_width), (REP, EXPERTS, CAP, share_width)
    ).reshape(N_EP, CAP, share_width)
    with jax.named_scope("route"):
        incoming = exchange(outgoing, EP).reshape(N_EP * CAP, share_width)

    with jax.named_scope("dense"):
        dense_held = lax.all_gather(extra[:, 256:], XC, axis=0).reshape(N_XC, N_Z, 16, 128)
    incoming, dense_held = lax.optimization_barrier((incoming, dense_held))
    tag = lax.dynamic_slice_in_dim(dense_held, 2 * xc_index, CAP, 2)[..., 96:98]
    tag = jnp.sum(tag.transpose(1, 0, 2, 3).reshape(N_EP * CAP, 2).astype(jnp.float32), axis=1)
    dense_held = dense_held.transpose(1, 0, 2, 3).reshape(width, 128)
    down = jnp.concatenate((expert_down[0], dense_held[:, 64:96].T), axis=0)
    dense_held = dense_held[:, :64]

    with jax.named_scope("join"):
        rows = gather_small(incoming, "tp", N_TP)
    rows, dense_held, down, tag, middle, combine_weights = lax.optimization_barrier(
        (rows, dense_held, down, tag, middle, combine_weights)
    )
    rows = rows.transpose(1, 0, 2).reshape(N_EP * CAP, width)
    branch_weight = jax.nn.sigmoid(jnp.sum(rows.astype(jnp.float32) * branch_gate, axis=1))
    dense_scale = branch_weight * tag

    def units(weight):
        return lax.dot_general(
            weight, rows, (((0,), (1,)), ((), ())), preferred_element_type=jnp.float32
        )

    hidden = (jax.nn.silu(units(expert_gate[0])) * units(expert_up[0])).astype(jnp.bfloat16)
    dense_both = units(dense_held)
    dense_hidden = (
        jax.nn.silu(dense_both[:32]) * dense_both[32:] * dense_scale[None]
    ).astype(jnp.bfloat16)
    all_hidden = jnp.concatenate((hidden, dense_hidden), axis=0)
    parts = lax.dot_general(
        all_hidden, down, (((0,), (0,)), ((), ())), preferred_element_type=jnp.float32
    ).astype(jnp.bfloat16)
    parts = parts.reshape(N_EP * CAP, N_TP, share_width).transpose(1, 0, 2)
    with jax.named_scope("reduce"):
        block_out = jnp.sum(exchange(parts, "tp").astype(jnp.float32), axis=0)
    block_out = block_out.astype(jnp.bfloat16).reshape(N_EP, CAP, share_width)
    with jax.named_scope("return"):
        returned = exchange(block_out, EP)
    expert_out = jnp.sum(
        returned.reshape(REP, EXPERTS * CAP, share_width).astype(jnp.float32), axis=0
    )
    routed = jnp.dot(combine_weights, expert_out, precision=lax.Precision.HIGHEST)
    return (middle + routed).astype(jnp.bfloat16)


def solution(mesh):
    fine = Mesh(mesh.devices.reshape(8, 2, 4, 2, 4), ("b", "zp", "x", "c", "tp"))
    return jax.shard_map(
        shards,
        mesh=fine,
        in_specs=(
            P(EP, None),
            P(),
            P(EP, "tp"),
            P(EP, "tp"),
            P(EP, "tp"),
            P(),
            P(),
            P("tp"),
            P(EP, "tp", None, None),
            P(EP, "tp", None, None),
            P(EP),
            P(),
            P("tp", EP),
            P(),
            P(EP, "tp"),
            P(EP, "tp"),
            P("tp", EP),
            P(),
            P(EP, None),
            P(EP, None),
            P(EP, None, "tp"),
            P(EP, None, "tp"),
            P(EP, "tp", None),
        ),
        out_specs=P(EP, "tp"),
        check_vma=False,
    )
```
